32 devices in a mesh: ep: 8 (over z, x), tp: 4 (over y, core).
Axes of the slice: x: 2, y: 2, z: 4, core: 2. Of those that a mesh axis runs over, the one named last changes fastest.
Arguments:
- queries: bfloat16 [4096, 2048], P('ep', 'tp'), may hold values from -6 to 6
- keys: bfloat16 [4096, 2048], P('ep', 'tp'), may hold values from -12 to 12
- values: bfloat16 [4096, 2048], P('ep', 'tp'), may hold values from -8 to 8
- key_bias: bfloat16 [4096, 16], P('ep', 'tp'), may hold values from -16 to 0
- out_weight: bfloat16 [2048, 2048], P('tp'), may hold values from -0.1875 to 0.1875
- moe_input: bfloat16 [1024, 2048], P('ep'), may hold values from -6 to 6
- moe_gain: float32 [2048], replicated, may hold values from 0.1 to 1.9
- route_ids: int32 [1024, 2], P('ep'), may hold values from 0 to 7, all different within a row; in each aligned block of 128 rows (0 to 127, 128 to 255, ...) at most 48 rows name the same one
- route_scores: float32 [1024, 2], P('ep'), may hold values from 0.05 to 1
- shared_gate: bfloat16 [2048, 2048], P(None, 'tp'), may hold values from -0.125 to 0.125
- shared_up: bfloat16 [2048, 2048], P(None, 'tp'), may hold values from -0.125 to 0.125
- shared_down: bfloat16 [2048, 2048], P('tp'), may hold values from -0.1875 to 0.1875
- expert_gate: bfloat16 [8, 2048, 2048], P('ep', None, 'tp'), may hold values from -0.125 to 0.125
- expert_up: bfloat16 [8, 2048, 2048], P('ep', None, 'tp'), may hold values from -0.125 to 0.125
- expert_down: bfloat16 [8, 2048, 2048], P('ep', 'tp'), may hold values from -0.1875 to 0.1875
Outputs:
- mixed_tokens: bfloat16 [4096, 2048], P('ep', 'tp')
- expert_mix: bfloat16 [1024, 2048], P('ep', 'tp')
The draws below stay inside these ranges and needn't reach their ends.
Inputs may be any that keep to these rules, and one draw needn't show every extreme that they name: `route_ids`: each row names 2 different experts. Among the 128 rows of one index of ep no expert is named by more than 48 rows, and in some such block one expert is named by exactly 48 rows.
All inputs are finite; a program needn't handle non-finite values.
Results may differ from the reference program's by a relative error of at most 0.019.
Values may be sent and summed in bfloat16 or wider, within the bound.
No kernel may reach another device: no remote copies, remote signals or barrier semaphores. Data moves between devices by JAX's collectives and lax.ppermute only.
A program may use at most 128 MiB of HBM per device.

```python
import math
import jax
import jax.numpy as jnp
import numpy as np
from jax import lax

D = 2048
HEADS = 16
HD = 128
F = 2048
FSH = 2048
TOPK = 2
SEQUENCE_COUNT = 1
ROWS_A = 512
ROWS_M = 128
ATTENTION_TOKENS = 4096
SEQUENCE_LENGTH = 4096
TOKENS_M = 1024
EXPERTS = 8
CAP = 48
N_EP = 8
N_TP = 4


def draw_key_bias(key, part):
    draw_keys = jax.random.split(key, 7)
    fast_share = 0.5
    fast_head = jax.random.uniform(draw_keys[0], (HEADS,)) < fast_share
    fast_rate = jnp.exp(jax.random.uniform(draw_keys[1], (HEADS,), minval=jnp.log(1.0 / 100.0), maxval=jnp.log(1.0 / 30.0)))
    slow_rate = jnp.exp(jax.random.uniform(draw_keys[2], (HEADS,), minval=jnp.log(0.3 / SEQUENCE_LENGTH), maxval=jnp.log(1.2 / SEQUENCE_LENGTH)))
    base_logit = jnp.log(jnp.where(fast_head, fast_rate, slow_rate)) - 2.15
    block_count = ATTENTION_TOKENS // ROWS_A
    block_shift = jax.random.uniform(draw_keys[3], (block_count, 1, HEADS), minval=-0.7, maxval=0.7)
    jitter = jax.random.uniform(draw_keys[4], (block_count, ROWS_A, HEADS), minval=-0.7, maxval=0.7)
    smoothing_factor = (base_logit[None, None, :] + block_shift + jitter).reshape(ATTENTION_TOKENS, HEADS)
    spike_position = jax.random.randint(draw_keys[5], (SEQUENCE_COUNT, 2), 0, SEQUENCE_LENGTH)
    token_position = jnp.arange(ATTENTION_TOKENS) % SEQUENCE_LENGTH
    sequence_index = jnp.arange(ATTENTION_TOKENS) // SEQUENCE_LENGTH
    spike_mask = jnp.any(token_position[:, None] == spike_position[sequence_index], axis=1)
    spike_fraction = jax.random.uniform(draw_keys[6], (ATTENTION_TOKENS, 1), minval=0.2, maxval=0.4)
    spike_logit = jnp.log(spike_fraction) - jnp.log(1.0 - spike_fraction)
    return jnp.where(spike_mask[:, None], spike_logit, smoothing_factor).astype(jnp.float32).astype(jnp.bfloat16)


def draw_values(key, part):
    draw_keys = jax.random.split(key, 3)
    block_count = ATTENTION_TOKENS // ROWS_A
    sign = jnp.where(jax.random.uniform(draw_keys[0], (HEADS,)) < 0.5, -1.0, 1.0)
    size = jax.random.uniform(draw_keys[1], (block_count, 1, HEADS, 1), minval=0.5, maxval=1.5)
    noise = jnp.clip(1.5 * jax.random.normal(draw_keys[2], (block_count, ROWS_A, HEADS, HD)), -6.0, 6.0)
    mixed = sign[None, None, :, None] * size + noise
    return mixed.reshape(ATTENTION_TOKENS, HEADS * HD).astype(jnp.float32).astype(jnp.bfloat16)


def with_spikes(array, rng, source, target, blocks, factor):
    def block_of(axis_at):
        return (jnp.arange(array.shape[axis_at]) // (array.shape[axis_at] // blocks)).reshape((-1,) + (1,) * (array.ndim - 1 - axis_at))

    one_side = jax.random.permutation(rng, blocks)[block_of(target)]
    far = (block_of(target) + blocks // 2) % blocks
    return jnp.where((block_of(source) == one_side) | (block_of(source) == far), factor * array, array)


def level_of(rng, extent, cuts, low, top_value):
    gain = 1.0
    for position, shards_of in cuts:
        heights = jax.random.uniform(jax.random.fold_in(jax.random.fold_in(rng, 6), position), (shards_of,), jnp.float32, low / len(cuts), top_value / len(cuts))
        gain = gain * jnp.repeat(jnp.exp(heights), extent[position] // shards_of).reshape((-1,) + (1,) * (len(extent) - 1 - position))
    return gain


def routed_block(key, own, number, rows, count, top, most, slope):
    order = jax.random.permutation(key, count)
    crowded, usual = portions_of(count, rows * top, most, slope, True), portions_of(count, rows * top, most, slope, False)
    places = jnp.arange(count)

    def named(lengths, offset_by):
        used = int((lengths > 0).sum())
        fixed = max(1, used // 4)
        shifted = fixed + (places - fixed + offset_by * (used - fixed)) % max(1, count - fixed)
        return jnp.zeros((count,), jnp.int32).at[order[jnp.where(places < fixed, places, shifted)]].set(jnp.asarray(lengths, jnp.int32))

    lengths = jnp.where(number % 4 == 0, named(crowded, number // 4), named(usual, number - number // 4 - 1))
    mixed = jax.random.permutation(jax.random.fold_in(own, 3), count)
    donor, sink = mixed[0:count // 2 * 2:2], mixed[1:count // 2 * 2:2]
    slack = jnp.minimum(lengths[donor] - 1, most - lengths[sink]) // 2
    slack = jnp.where((donor == order[0]) | (sink == order[0]) | (lengths[sink] == 0), 0, jnp.maximum(slack, 0))
    shifted = jax.random.randint(jax.random.fold_in(own, 4), (count // 2,), 0, 1 << 20) % (slack + 1)
    lengths = lengths.at[donor].add(-shifted).at[sink].add(shifted)
    members = jnp.searchsorted(jnp.cumsum(lengths), jnp.arange(rows * top), side="right").astype(jnp.int32)
    table = members.reshape(top, rows).T
    table = table[jax.random.permutation(jax.random.fold_in(own, 1), rows)]
    offset_by = jax.random.randint(jax.random.fold_in(own, 2), (rows, 1), 0, top)
    return jnp.take_along_axis(table, (jnp.arange(top)[None, :] + offset_by) % top, axis=1)


def portions_of(count, total, limit, lean, full):
    portions = [(1 << 20) // math.isqrt(standing ** lean) + 1 for standing in range(1, count + 1)]
    largest = limit if full else min(limit, max(-(-total // count), total * portions[0] // sum(portions)))
    least = 1 if total - largest >= count - 1 else 0
    holding, surplus = [largest] + [least] * (count - 1), total - largest - least * (count - 1)
    while surplus > 0:
        free = [i for i in range(1, count) if holding[i] < largest] or [i for i in range(1, count) if holding[i] < limit]
        mass, left = sum([portions[i] for i in free]), surplus
        for i in free:
            extra = min(limit - holding[i], max(1, left * portions[i] // mass), surplus)
            holding[i] = holding[i] + extra
            surplus = surplus - extra
    return np.array(holding)


def centred(rng, extent, deviation, most, shards=(), kind=jnp.bfloat16):
    gain = level_of(rng, extent, shards, -0.22, 0.18) if shards else 1.0
    values = jax.random.normal(rng, extent, jnp.float32) * deviation * gain
    return jnp.minimum(jnp.maximum(values, -most), most).astype(kind)


def gaussian_with(stream_key, dims, scale, limit, shards, heavy, held_as=jnp.bfloat16):
    array = scale * jax.random.normal(stream_key, dims, jnp.float32)
    if shards:
        array = array * level_of(stream_key, dims, shards, -0.22, 0.18)
    return jnp.clip(with_spikes(array, jax.random.fold_in(stream_key, 3), *heavy), -limit, limit).astype(held_as)


def setup_inputs(seed: int = 0) -> dict:
    streams_of = jax.random.split(jax.random.key(seed), 16)
    queries = centred(streams_of[0], (ATTENTION_TOKENS, HEADS * HD), 1.0, 6.0, ((0, 8), (1, 4)))
    keys = centred(streams_of[1], (ATTENTION_TOKENS, HEADS * HD), 2.0, 12.0, ((0, 8), (1, 4)))
    values = draw_values(jax.random.fold_in(streams_of[15], 71), 0)
    key_bias = draw_key_bias(jax.random.fold_in(streams_of[15], 71), 0)
    out_weight = gaussian_with(streams_of[4], (HEADS * HD, D), (HEADS * HD) ** -0.5, 0.1875, ((0, 4),), (0, 1, 4, 2.0))
    moe_input = centred(streams_of[5], (TOKENS_M, D), 1.0, 6.0, ((0, 8),))
    moe_gain = jnp.clip(1.0 + 0.18 * jax.random.normal(streams_of[6], (D,), jnp.float32), 0.1, 1.9)
    route_ids_keys = jax.random.split(jax.random.fold_in(streams_of[7], 1), TOKENS_M // ROWS_M)
    route_ids_turns = jax.random.permutation(jax.random.fold_in(streams_of[7], 3), TOKENS_M // ROWS_M)
    route_ids = jax.vmap(lambda own, number: routed_block(jax.random.fold_in(streams_of[7], 2), own, number, ROWS_M, EXPERTS, TOPK, CAP, 2))(route_ids_keys, route_ids_turns).reshape((TOKENS_M, TOPK))
    route_scores = jnp.clip(0.05 + 0.95 * jax.random.uniform(streams_of[8], (TOKENS_M, TOPK), jnp.float32) ** level_of(streams_of[8], (TOKENS_M, TOPK), ((0, 8),), -0.2, 0.2), 0.05, 1.0)
    shared_gate = centred(streams_of[9], (D, FSH), D ** -0.5, 0.125, ((1, 4),))
    shared_up = centred(streams_of[10], (D, FSH), D ** -0.5, 0.125, ((1, 4),))
    shared_down = gaussian_with(streams_of[11], (FSH, D), FSH ** -0.5, 0.1875, ((0, 4),), (0, 1, 4, 2.0))
    expert_gate = centred(streams_of[12], (EXPERTS, D, F), D ** -0.5, 0.125, ((0, 8), (2, 4)))
    expert_up = centred(streams_of[13], (EXPERTS, D, F), D ** -0.5, 0.125, ((0, 8), (2, 4)))
    expert_down = gaussian_with(streams_of[14], (EXPERTS, F, D), F ** -0.5, 0.1875, ((0, 8), (1, 4)), (1, 2, 4, 2.0))
    return {"queries": queries, "keys": keys, "values": values, "key_bias": key_bias, "out_weight": out_weight, "moe_input": moe_input, "moe_gain": moe_gain, "route_ids": route_ids, "route_scores": route_scores, "shared_gate": shared_gate, "shared_up": shared_up, "shared_down": shared_down, "expert_gate": expert_gate, "expert_up": expert_up, "expert_down": expert_down}


EPS_NORM = 1e-06
ROUTED_SCALE = 2.5

def head_span(query_head, key_head, value_head, bias_head):
    length = query_head.shape[0]
    block = min(512, length)
    scale = HD ** (-0.5)
    key_pos = jnp.arange(length, dtype=jnp.int32)
    bias_row = bias_head.astype(jnp.float32)[None, :]

    def one_block(start):
        query_block = lax.dynamic_slice_in_dim(query_head, start, block, 0)
        logit = jnp.dot(query_block, key_head.T, preferred_element_type=jnp.float32) * scale + bias_row
        query_pos = start + jnp.arange(block, dtype=jnp.int32)
        visible = key_pos[None, :] < query_pos[:, None]
        keep = jnp.where(visible, jax.nn.log_sigmoid(-logit), 0.0)
        stay = lax.cumsum(keep, axis=1, reverse=True) - keep
        weight = jnp.where(visible, jnp.exp(jax.nn.log_sigmoid(logit) + stay), 0.0).astype(jnp.bfloat16)
        return jnp.dot(weight, value_head, preferred_element_type=jnp.float32).astype(jnp.bfloat16)
    starts = jnp.arange(length // block, dtype=jnp.int32) * block
    return lax.map(one_block, starts).reshape(length, -1)

def per_head(operands):
    return head_span(operands[0], operands[1], operands[2], operands[3])

def grouped_sum(left, right, groups):
    width = left.shape[1] // groups
    total = jnp.zeros((left.shape[0], right.shape[1]), jnp.float32)
    for group in range(groups):
        partial_sum = jnp.dot(left[:, group * width:(group + 1) * width], right[group * width:(group + 1) * width], preferred_element_type=jnp.float32)
        rounded = lax.optimization_barrier(partial_sum.astype(jnp.bfloat16))
        total = total + rounded.astype(jnp.float32)
    return total

def one_expert(operands):
    rows_in, weight_gate, weight_up, weight_down = operands
    gate_part = jnp.dot(rows_in, weight_gate, preferred_element_type=jnp.float32)
    up_part = jnp.dot(rows_in, weight_up, preferred_element_type=jnp.float32)
    hidden = (jax.nn.silu(gate_part) * up_part).astype(jnp.bfloat16)
    return grouped_sum(hidden, weight_down, N_TP).astype(jnp.bfloat16)

def reference(queries, keys, values, key_bias, out_weight, moe_input, moe_gain, route_ids, route_scores, shared_gate, shared_up, shared_down, expert_gate, expert_up, expert_down):
    pieces = []
    for sequence_index in range(SEQUENCE_COUNT):
        first = sequence_index * SEQUENCE_LENGTH
        query_seq = queries[first:first + SEQUENCE_LENGTH].reshape(SEQUENCE_LENGTH, HEADS, HD).transpose(1, 0, 2)
        key_seq = keys[first:first + SEQUENCE_LENGTH].reshape(SEQUENCE_LENGTH, HEADS, HD).transpose(1, 0, 2)
        value_seq = values[first:first + SEQUENCE_LENGTH].reshape(SEQUENCE_LENGTH, HEADS, HD).transpose(1, 0, 2)
        bias_seq = key_bias[first:first + SEQUENCE_LENGTH].T
        head_outs = lax.map(per_head, (query_seq, key_seq, value_seq, bias_seq))
        pieces.append(head_outs.transpose(1, 0, 2).reshape(SEQUENCE_LENGTH, HEADS * HD))
    heads_out = jnp.concatenate(pieces, axis=0)
    mixed_tokens = grouped_sum(heads_out, out_weight, N_TP).astype(jnp.bfloat16)
    inputs = moe_input.astype(jnp.float32)
    normed = (inputs * lax.rsqrt(lax.optimization_barrier(jnp.mean(inputs * inputs, axis=-1, keepdims=True)) + EPS_NORM) * moe_gain.astype(jnp.float32)).astype(jnp.bfloat16)
    shared_hidden = (jax.nn.silu(jnp.dot(normed, shared_gate, preferred_element_type=jnp.float32)) * jnp.dot(normed, shared_up, preferred_element_type=jnp.float32)).astype(jnp.bfloat16)
    shared_result = grouped_sum(shared_hidden, shared_down, N_TP)
    chosen = route_ids.reshape(N_EP, ROWS_M * TOPK).astype(jnp.int32)
    onehot = (chosen[:, :, None] == jnp.arange(EXPERTS, dtype=jnp.int32)[None, None, :]).astype(jnp.int32)
    place = lax.optimization_barrier(jnp.sum((jnp.cumsum(onehot, axis=1) - onehot) * onehot, axis=2))
    block_ids = jnp.arange(N_EP, dtype=jnp.int32)[:, None]
    slot_index = (chosen * (N_EP * CAP) + block_ids * CAP + place).reshape(-1).astype(jnp.int32)
    token_index = jnp.arange(TOKENS_M * TOPK, dtype=jnp.int32) // TOPK
    expert_rows = jnp.zeros((EXPERTS * N_EP * CAP, D), jnp.bfloat16).at[slot_index].set(normed[token_index])
    expert_rows = expert_rows.reshape(EXPERTS, N_EP * CAP, D)
    results = lax.map(one_expert, (expert_rows, expert_gate, expert_up, expert_down))
    results = results.reshape(EXPERTS * N_EP * CAP, D)
    picked = results[slot_index].astype(jnp.float32).reshape(TOKENS_M, TOPK, D)
    scores = route_scores.astype(jnp.float32)
    gates = scores / lax.optimization_barrier(jnp.sum(scores, axis=-1, keepdims=True)) * ROUTED_SCALE
    expert_mix = (shared_result + lax.optimization_barrier(jnp.sum(gates[:, :, None] * picked, axis=1))).astype(jnp.bfloat16)
    return (mixed_tokens, expert_mix)
```

```python
import functools

import jax
import jax.numpy as jnp
from jax import lax
from jax.experimental import pallas as pl
from jax.experimental.pallas import tpu as pltpu
from jax.sharding import PartitionSpec as P

SEQUENCE_COUNT = 1


EPS_NORM = 1e-06
ROUTED_SCALE = 2.5
LOG2E = 1.4426950408889634


def partner_2(array, axis, apart):
    return lax.ppermute(array, axis, [(i, i ^ 1 << apart) for i in range(lax.axis_size(axis))])


def swap(array, axis, mask):
    return lax.ppermute(array, axis, [(i, i ^ mask) for i in range(lax.axis_size(axis))])


def stick_kernel(scale, half_ref, own_ref, other_ref, q_ref, out_ref, k_s, v_s, b_s, tri_s, acc_s, carry_s):
    blocks, rows, width = q_ref.shape
    bias_rows = rows // width
    mine = half_ref[0]
    for which, ref in ((mine, own_ref), (1 - mine, other_ref)):
        k_s[which] = ref[:, :rows]
        v_s[which] = ref[:, rows : 2 * rows]
        for block in range(blocks):
            lanes = [
                ref[block, pl.ds(2 * rows + r, 1), :].astype(jnp.float32) * LOG2E
                for r in range(bias_rows)
            ]
            b_s[which, block] = jnp.concatenate(lanes, axis=1)
    later = lax.broadcasted_iota(jnp.int32, (rows, rows + width), 0)
    column = lax.broadcasted_iota(jnp.int32, (rows, rows + width), 1)
    tri_s[...] = jnp.where((later > column) | (column >= rows), 1.0, 0.0).astype(jnp.bfloat16)

    def step(query, source, visible_of):
        for part in (1, 0):
            logit = lax.dot_general(
                query,
                k_s[part, source],
                (((1,), (1,)), ((), ())),
                preferred_element_type=jnp.float32,
            )
            logit = logit * scale + b_s[part, source]
            soft = jnp.maximum(logit, jnp.log2(1.0 + jnp.exp2(jnp.minimum(logit, 64.0))))
            if visible_of is not None:
                visible = visible_of(part)
                soft = jnp.where(visible, soft, 0.0)
            sums = jnp.dot(soft.astype(jnp.bfloat16), tri_s[...], preferred_element_type=jnp.float32)
            carry = carry_s[...]
            carry_s[...] = carry + sums[:, rows:]
            wide = jnp.concatenate([carry] * bias_rows, axis=1)
            weight = jnp.exp2((logit - soft) - (sums[:, :rows] + wide))
            if visible_of is not None:
                weight = jnp.where(visible, weight, 0.0)
            acc_s[...] += jnp.dot(
                weight.astype(jnp.bfloat16), v_s[part, source], preferred_element_type=jnp.float32
            )

    def one_block(block, _):
        query = q_ref[block]
        acc_s[...] = jnp.zeros_like(acc_s)
        carry_s[...] = jnp.zeros_like(carry_s)
        row = lax.broadcasted_iota(jnp.int32, (rows, rows), 0) + mine * rows
        key = lax.broadcasted_iota(jnp.int32, (rows, rows), 1)
        step(query, block, lambda part: key + part * rows < row)

        def earlier(turn, _):
            step(query, block - 1 - turn, None)
            return 0

        lax.fori_loop(0, block, earlier, 0)
        out_ref[block] = acc_s[...].astype(out_ref.dtype)
        return 0

    lax.fori_loop(0, blocks, one_block, 0)


def stick(half, own, other, query):
    blocks, rows, width = query.shape
    pairs = blocks * (blocks + 1) * rows * rows
    vmem = pl.BlockSpec(memory_space=pltpu.VMEM)
    return pl.pallas_call(
        functools.partial(stick_kernel, width**-0.5 * LOG2E),
        out_shape=jax.ShapeDtypeStruct(query.shape, jnp.bfloat16),
        in_specs=[pl.BlockSpec(memory_space=pltpu.SMEM), vmem, vmem, vmem],
        out_specs=vmem,
        scratch_shapes=[
            pltpu.VMEM((2, blocks, rows, width), jnp.bfloat16),
            pltpu.VMEM((2, blocks, rows, width), jnp.bfloat16),
            pltpu.VMEM((2, blocks, 1, rows), jnp.float32),
            pltpu.VMEM((rows, rows + width), jnp.bfloat16),
            pltpu.VMEM((rows, width), jnp.float32),
            pltpu.VMEM((rows, width), jnp.float32),
        ],
        cost_estimate=pl.CostEstimate(
            flops=2 * pairs * (rows + 3 * width),
            bytes_accessed=12 * blocks * rows * width,
            transcendentals=3 * pairs,
        ),
        name="stick",
    )(half, own, other, query)


def by_group(core, own, other, axis=0):
    return jnp.where(
        core == 0, jnp.concatenate([own, other], axis), jnp.concatenate([other, own], axis)
    )


def head_attention(queries, keys, values, key_bias, out_weight):
    span, width = queries.shape
    heads = key_bias.shape[1]
    depth = width // heads
    half = span // 2
    ep_count = lax.axis_size("ep")
    tp_count = lax.axis_size("tp")
    tp_index = lax.axis_index("tp")
    core = tp_index % 2
    pad = 16 - half // depth % 16

    def split(array):
        return (
            lax.dynamic_slice_in_dim(array, core * half, half, 0),
            lax.dynamic_slice_in_dim(array, (1 - core) * half, half, 0),
        )

    def per_head(array):
        return array.reshape(half, heads, depth).transpose(1, 0, 2)

    own, away = zip(*[split(array) for array in (keys, values, queries, key_bias)])
    got = [swap(array, "tp", 1) for array in away]

    def bias_rows(array):
        rows = array.T.reshape(heads, half // depth, depth)
        return jnp.pad(rows, ((0, 0), (0, pad), (0, 0)))

    def key_message(key_rows, value_rows, bias):
        return jnp.concatenate([per_head(key_rows), per_head(value_rows), bias_rows(bias)], axis=1)

    key_parts = by_group(
        core, key_message(own[0], own[1], own[3]), key_message(got[0], got[1], got[3])
    )
    query_parts = by_group(core, per_head(own[2]), per_head(got[2]))
    own_keys = lax.all_to_all(key_parts, "ep", split_axis=0, concat_axis=0, tiled=True)
    query_rows = lax.all_to_all(query_parts, "ep", split_axis=0, concat_axis=0, tiled=True)
    other_keys = swap(own_keys, "tp", 1)
    out = stick(core.reshape(1), own_keys, other_keys, query_rows)
    back = lax.all_to_all(out, "ep", split_axis=0, concat_axis=0, tiled=True)
    other_weight = swap(out_weight, "tp", 1)

    def project(group, weight):
        rows = lax.dynamic_slice_in_dim(back, group * heads, heads, 0)
        return jnp.dot(
            rows.transpose(1, 0, 2).reshape(half, width), weight, preferred_element_type=jnp.float32
        )

    partial = (project(core, out_weight) + project(1 - core, other_weight)).astype(jnp.bfloat16)
    cols = partial.shape[1] // tp_count

    def columns(index):
        return lax.dynamic_slice_in_dim(partial, index * cols, cols, 1)

    same = columns(tp_index).astype(jnp.float32)
    cross = jnp.zeros_like(same)
    for mask in range(1, tp_count):
        piece = swap(columns(tp_index ^ mask), "tp", mask).astype(jnp.float32)
        if mask % 2:
            cross = cross + piece
        else:
            same = same + piece
    return by_group(core, same.astype(jnp.bfloat16), cross.astype(jnp.bfloat16))


def absorb(state, query_heads, piece, visible):
    total, carried = state
    key_piece, value_piece, bias_piece = piece
    span = key_piece.shape[0]
    heads = query_heads.shape[1]
    key_heads = key_piece.reshape(span, heads, -1)
    value_heads = value_piece.reshape(span, heads, -1)
    scale = query_heads.shape[2] ** (-0.5)
    logit = (
        jnp.einsum("qhd,khd->hqk", query_heads, key_heads, preferred_element_type=jnp.float32)
        * scale
    )
    logit = logit + bias_piece.astype(jnp.float32).T[:, None, :]
    keep = jnp.where(visible[None], jax.nn.log_sigmoid(-logit), 0.0)
    stay = lax.cumsum(keep, axis=2, reverse=True) - keep + carried[:, :, None]
    weight = jnp.where(visible[None], jnp.exp(jax.nn.log_sigmoid(logit) + stay), 0.0).astype(
        jnp.bfloat16
    )
    total = total + jnp.einsum(
        "hqk,khd->qhd", weight, value_heads, preferred_element_type=jnp.float32
    )
    return (total, carried + jnp.sum(keep, axis=2))


def fresh_state(query_heads):
    return (
        jnp.zeros(query_heads.shape, jnp.float32),
        jnp.zeros((query_heads.shape[1], query_heads.shape[0]), jnp.float32),
    )


def diagonal(query_heads, piece, offset):
    count = query_heads.shape[0]
    span = piece[0].shape[0]
    key_pos = jnp.arange(span, dtype=jnp.int32)
    query_pos = offset + jnp.arange(count, dtype=jnp.int32)
    visible = key_pos[None, :] < query_pos[:, None]
    return absorb(fresh_state(query_heads), query_heads, piece, visible)


def row_attention(queries, keys, values, key_bias, out_weight):
    span = queries.shape[0]
    heads = key_bias.shape[1]
    query_heads = queries.reshape(span, heads, -1)
    ep_count = lax.axis_size("ep")
    seq_devices = ep_count // SEQUENCE_COUNT
    own_index = lax.axis_index("ep")
    place = own_index % seq_devices
    own_piece = (keys, values, key_bias)
    half = span // 2
    group_bits = seq_devices.bit_length() - 1

    def mirror(rows):
        for bit in range(group_bits):
            rows = partner_2(rows, "ep", bit)
        return rows

    whole = (
        lax.all_gather(own_piece[0], "ep", axis=0, tiled=True),
        lax.all_gather(own_piece[1], "ep", axis=0, tiled=True),
        lax.all_gather(own_piece[2], "ep", axis=0, tiled=True),
    )
    mirror_place = seq_devices - 1 - place
    mirror_index = own_index - place + mirror_place
    early_rows = query_heads[:half]
    late_rows = mirror(queries[half:]).reshape(half, heads, -1)
    partner = tuple(
        (lax.dynamic_slice_in_dim(member, mirror_index * span, span, 0) for member in whole)
    )
    half_visible = jnp.ones((half, span), jnp.bool_)

    def unchanged(inner):
        return inner

    def visit_both(turn, carry):
        early, late = carry
        early_source = jnp.maximum(own_index - turn, 0)
        late_source = jnp.maximum(mirror_index - turn, 0)
        early_piece = tuple(
            (lax.dynamic_slice_in_dim(member, early_source * span, span, 0) for member in whole)
        )
        late_piece = tuple(
            (lax.dynamic_slice_in_dim(member, late_source * span, span, 0) for member in whole)
        )

        def early_taken(inner):
            return absorb(inner, early_rows, early_piece, half_visible)

        def late_taken(inner):
            return absorb(inner, late_rows, late_piece, half_visible)

        early = lax.cond(place >= turn, early_taken, unchanged, early)
        late = lax.cond(mirror_place >= turn, late_taken, unchanged, late)
        return (early, late)

    early_state, late_state = lax.fori_loop(
        1,
        seq_devices,
        visit_both,
        (diagonal(early_rows, own_piece, 0), diagonal(late_rows, partner, half)),
    )
    early_out = early_state[0].astype(jnp.bfloat16).reshape(half, -1)
    late_out = mirror(late_state[0].astype(jnp.bfloat16).reshape(half, -1))
    heads_out = jnp.concatenate([early_out, late_out], axis=0)
    summed = lax.psum_scatter(
        jnp.dot(heads_out, out_weight, preferred_element_type=jnp.float32).astype(jnp.bfloat16),
        "tp",
        scatter_dimension=1,
        tiled=True,
    )
    return summed


def gather_columns(piece):
    count = lax.axis_size("tp")
    index = lax.axis_index("tp")
    cols = piece.shape[1]
    whole = jnp.zeros((piece.shape[0], count * cols), piece.dtype)
    held = [(0, piece)]
    for bit in reversed(range(count.bit_length() - 1)):
        held = held + [(mask | 1 << bit, swap(part, "tp", 1 << bit)) for mask, part in held]
    for mask, part in held:
        whole = lax.dynamic_update_slice(whole, part, (0, (index ^ mask) * cols))
    return whole


def scatter_sum(partial):
    count = lax.axis_size("tp")
    index = lax.axis_index("tp")
    rows = partial.shape[0]
    parts = partial.reshape(rows, count, -1)
    for bit in range(count.bit_length() - 1):
        mine = index >> bit & 1
        parts = parts.reshape(rows, parts.shape[1] // 2, 2, parts.shape[2])
        kept = lax.dynamic_index_in_dim(parts, mine, 2, False)
        sent = lax.dynamic_index_in_dim(parts, 1 - mine, 2, False)
        parts = kept.astype(jnp.float32) + swap(sent.astype(jnp.bfloat16), "tp", 1 << bit)
    return parts.reshape(rows, -1)


def expert_layer(
    moe_input,
    moe_gain,
    route_ids,
    route_scores,
    shared_gate,
    shared_up,
    shared_down,
    expert_gate,
    expert_up,
    expert_down,
):
    ep_count = lax.axis_size("ep")
    token_count, width = moe_input.shape
    cols = width // lax.axis_size("tp")
    inputs = moe_input.astype(jnp.float32)
    normed = (
        inputs * lax.rsqrt(jnp.mean(inputs * inputs, axis=-1, keepdims=True) + EPS_NORM) * moe_gain
    ).astype(jnp.bfloat16)
    own_cols = lax.dynamic_slice_in_dim(normed, lax.axis_index("tp") * cols, cols, 1)
    local_experts = expert_gate.shape[0]
    expert_count = local_experts * ep_count
    topk = route_ids.shape[1]
    capacity = 3 * token_count * topk // (2 * expert_count)
    slots = expert_count * capacity
    pairs = token_count * topk
    chosen = route_ids.reshape(-1)
    pair_at = jnp.arange(pairs, dtype=jnp.int32)
    earlier = (chosen[:, None] == chosen[None, :]) & (pair_at[None, :] < pair_at[:, None])
    place_in = jnp.sum(earlier.astype(jnp.int32), axis=1)
    slot_ids = (chosen * capacity + place_in).reshape(token_count, topk)
    slot_at = jnp.arange(slots, dtype=jnp.int32)
    picks = [(slot_ids[:, k, None] == slot_at[None, :]) for k in range(topk)]
    dispatch = functools.reduce(jnp.logical_or, picks).astype(jnp.bfloat16)
    outgoing = lax.dot_general(
        dispatch, own_cols, (((0,), (0,)), ((), ())), preferred_element_type=jnp.float32
    ).astype(jnp.bfloat16)
    arrived = lax.all_to_all(outgoing, "ep", split_axis=0, concat_axis=0, tiled=True)
    piece = gather_columns(arrived)
    shared_hidden = (
        jax.nn.silu(jnp.dot(normed, shared_gate, preferred_element_type=jnp.float32))
        * jnp.dot(normed, shared_up, preferred_element_type=jnp.float32)
    ).astype(jnp.bfloat16)
    common = jnp.dot(shared_hidden, shared_down, preferred_element_type=jnp.float32)
    if local_experts == 1:
        grid = piece
        gate_sum = jnp.dot(grid, expert_gate[0], preferred_element_type=jnp.float32)
        up_sum = jnp.dot(grid, expert_up[0], preferred_element_type=jnp.float32)
        expert_hidden = (jax.nn.silu(gate_sum) * up_sum).astype(jnp.bfloat16)
        routed = jnp.dot(expert_hidden, expert_down[0], preferred_element_type=jnp.float32)
    else:
        grid = piece.reshape(ep_count, local_experts, capacity, width)
        gate_sum = jnp.einsum("secd,edf->secf", grid, expert_gate, preferred_element_type=jnp.float32)
        up_sum = jnp.einsum("secd,edf->secf", grid, expert_up, preferred_element_type=jnp.float32)
        expert_hidden = (jax.nn.silu(gate_sum) * up_sum).astype(jnp.bfloat16)
        routed = jnp.einsum(
            "secf,efd->secd", expert_hidden, expert_down, preferred_element_type=jnp.float32
        ).reshape(slots, width)
    summed = scatter_sum(jnp.concatenate([routed, common], axis=0).astype(jnp.bfloat16))
    returned = lax.all_to_all(
        summed[:slots].astype(jnp.bfloat16), "ep", split_axis=0, concat_axis=0, tiled=True
    )
    gates = route_scores / jnp.sum(route_scores, axis=-1, keepdims=True) * ROUTED_SCALE
    mix = summed[slots:]
    for k in range(topk):
        row = jnp.dot(picks[k].astype(jnp.bfloat16), returned, preferred_element_type=jnp.float32)
        mix = mix + row * gates[:, k, None]
    return mix.astype(jnp.bfloat16)


def body(
    queries,
    keys,
    values,
    key_bias,
    out_weight,
    *moe,
):
    ep_count = lax.axis_size("ep")
    if SEQUENCE_COUNT == 1 and 2 * key_bias.shape[1] == ep_count and lax.axis_size("tp") % 2 == 0:
        mixed = head_attention(queries, keys, values, key_bias, out_weight)
    else:
        mixed = row_attention(queries, keys, values, key_bias, out_weight)
    return (mixed, expert_layer(*moe))


def solution(mesh):
    return jax.shard_map(
        body,
        mesh=mesh,
        in_specs=(
            P("ep", "tp"),
            P("ep", "tp"),
            P("ep", "tp"),
            P("ep", "tp"),
            P("tp", None),
            P("ep", None),
            P(),
            P("ep", None),
            P("ep", None),
            P(None, "tp"),
            P(None, "tp"),
            P("tp", None),
            P("ep", None, "tp"),
            P("ep", None, "tp"),
            P("ep", "tp", None),
        ),
        out_specs=(P("ep", "tp"), P("ep", "tp")),
        check_vma=False,
    )
```

```python
import functools

import jax
import jax.numpy as jnp
import numpy as np
from jax import lax
from jax.experimental import pallas as pl
from jax.experimental.pallas import tpu as pltpu
from jax.sharding import PartitionSpec as P


SEQUENCE_COUNT = 1


EPS_NORM = 1e-06
ROUTED_SCALE = 2.5
LOG2E = 1.4426950408889634
NEVER = -1e30
MIB = 1 << 20


def partner_2(array, axis, apart):
    return lax.ppermute(array, axis, [(i, i ^ 1 << apart) for i in range(lax.axis_size(axis))])


def swap(array, axis, mask):
    return lax.ppermute(array, axis, [(i, i ^ mask) for i in range(lax.axis_size(axis))])


def rounds_of(heads):
    return [(k, s) for k in range(heads) for s in range(2)]


def send_round(array, heads, k, s):
    ep_count, tp_count = lax.axis_size("ep"), lax.axis_size("tp")
    pairs = []
    for i in range(ep_count):
        for t in range(tp_count):
            core = t % 2
            to_ep = core * heads + (i + k) % heads
            to_tp = t - core + (i // heads + s) % 2
            pairs.append((i * tp_count + t, to_ep * tp_count + to_tp))
    return lax.ppermute(array, ("ep", "tp"), pairs)


def pack_kernel(heads, k_ref, v_ref, q_ref, bias_ref, *refs):
    out_refs, bias_s = refs[:-1], refs[-1]
    own = lax.axis_index("ep")
    span = k_ref.shape[0]
    half = span // 2
    depth = k_ref.shape[1] // heads
    bias_rows = half // depth
    turned = bias_ref[...].astype(jnp.float32)
    for head in range(heads):
        for r in range(span // depth):
            bias_s[head, r] = turned[head : head + 1, r * depth : (r + 1) * depth]
    for (k, s), out_ref in zip(rounds_of(heads), out_refs):
        head = lax.rem(own + k, heads)
        part = lax.rem(own // heads + s, 2)
        rows = pl.ds(pl.multiple_of(part * half, half), half)
        lanes = pl.ds(pl.multiple_of(head * depth, depth), depth)
        out_ref[:half] = k_ref[rows, lanes]
        out_ref[half : 2 * half] = v_ref[rows, lanes]
        pad = out_ref.shape[0] - 3 * half
        at = lax.broadcasted_iota(jnp.int32, (pad, depth), 0)
        bias = jnp.zeros((pad, depth), jnp.float32)
        for r in range(bias_rows):
            bias = jnp.where(at == r, bias_s[head, part * bias_rows + r], bias)
        out_ref[2 * half : 2 * half + pad] = bias.astype(out_ref.dtype)
        out_ref[2 * half + pad :] = q_ref[rows, lanes]


def pack(keys, values, queries, bias):
    heads, span = bias.shape
    half, depth = span // 2, keys.shape[1] // heads
    pad = -(-(half // depth) // 16) * 16
    vmem = pl.BlockSpec(memory_space=pltpu.VMEM)
    count = len(rounds_of(heads))
    shape = jax.ShapeDtypeStruct((3 * half + pad, depth), keys.dtype)
    return pl.pallas_call(
        functools.partial(pack_kernel, heads),
        out_shape=[shape] * count,
        in_specs=[vmem] * 4,
        out_specs=[vmem] * count,
        scratch_shapes=[pltpu.VMEM((heads, span // depth, 1, depth), jnp.float32)],
        cost_estimate=pl.CostEstimate(
            flops=keys.size * 8, bytes_accessed=12 * keys.size, transcendentals=0
        ),
        name="pack",
    )(keys, values, queries, bias)


def steps_of(groups, turns):
    steps = [(g, source) for g in range(groups) for source in reversed(range((g + 1) * turns))]
    return steps + [(groups, 0)] * 2


def stick_kernel(scale, heads, turn, turns, spot, table_ref, *refs):
    count = 2 * heads
    messages, out_ref = refs[: 2 * count], refs[2 * count]
    mes_s, q_s, b_s, tri_s, reach_s, soft_s, log_s, prod_s, acc_s, carry_s, sems = refs[2 * count + 1 :]
    blocks, piece, width = out_ref.shape
    groups = blocks // turns
    rows = piece * turns
    bias_rows = rows // width
    pad = mes_s.shape[2] - 3 * rows
    place, mine = spot()
    for at, which in enumerate((mine, 1 - mine)):
        for (k, s), ref in zip(rounds_of(heads), messages[at * count : (at + 1) * count]):
            block = lax.rem(which + s, 2) * heads + lax.rem(place + heads - k, heads)
            pltpu.make_async_copy(ref, mes_s.at[which, block], sems.at[which, block]).start()
    later = lax.broadcasted_iota(jnp.int32, (2 * rows, rows), 0)
    column = lax.broadcasted_iota(jnp.int32, (2 * rows, rows), 1)
    tri_s[...] = jnp.where(later > column, 1.0, 0.0).astype(jnp.bfloat16)
    row = lax.broadcasted_iota(jnp.int32, (rows, rows), 0)
    row = row // piece * (2 * rows) + row % piece + (mine * rows + turn * piece)
    reach_s[...] = lax.broadcasted_iota(jnp.int32, (rows, rows), 1) - row
    query_at = 2 * rows + pad + turn * piece

    def arrive(group):
        for at in range(turns):
            block = group * turns + at
            for which in (0, 1):
                pltpu.make_async_copy(
                    messages[0], mes_s.at[which, block], sems.at[which, block]
                ).wait()
                lanes = [
                    mes_s[which, block, 2 * rows + r : 2 * rows + r + 1, :].astype(jnp.float32)
                    for r in range(bias_rows)
                ]
                b_s[which, block] = jnp.concatenate(lanes, axis=1) * LOG2E
            q_s[group, at * piece : (at + 1) * piece] = mes_s[
                mine, block, query_at : query_at + piece
            ]

    arrive(0)
    arrive(1)
    q_s[groups] = q_s[0]
    parts = (1, 0)

    def scores(group, source):
        return [
            lax.dot_general(
                q_s[group],
                mes_s[part, source, :rows],
                (((1,), (1,)), ((), ())),
                preferred_element_type=jnp.float32,
            )
            for part in parts
        ]

    def soften(slot, group, source):
        ahead = (group * turns - source) * (2 * rows)
        for part in parts:
            logit = prod_s[part] * scale + b_s[part, source]
            logit = jnp.where(reach_s[...] < ahead - part * rows, logit, NEVER)
            soft = jnp.maximum(logit, jnp.log2(1.0 + jnp.exp2(jnp.minimum(logit, 64.0))))
            soft_s[slot, part] = soft.astype(jnp.bfloat16)
            log_s[slot, part] = logit - soft

    def sums(slot):
        one = jnp.dot(soft_s[slot, 1], tri_s[:rows], preferred_element_type=jnp.float32)
        both = jnp.concatenate([soft_s[slot, 0], soft_s[slot, 1]], axis=1)
        return [one, jnp.dot(both, tri_s[...], preferred_element_type=jnp.float32)]

    def entry(t):
        return table_ref[0, 2 * t], table_ref[0, 2 * t + 1]

    def put(products):
        for part, product in zip(parts, products):
            prod_s[part] = product

    put(scores(*entry(0)))
    soften(0, *entry(0))
    put(scores(*entry(1)))

    def pair(at, _):
        acc = acc_s[...]
        carry = carry_s[...]
        for slot in range(2):
            t = 2 * at + slot
            totals = sums(slot)
            products = scores(*entry(t + 2))
            soften(1 - slot, *entry(t + 1))
            put(products)
            wide = jnp.concatenate([carry] * bias_rows, axis=1)
            source = entry(t)[1]
            for part, total in zip(parts, totals):
                weight = jnp.exp2(log_s[slot, part] - (total + wide)).astype(jnp.bfloat16)
                values = mes_s[part, source, rows : 2 * rows]
                acc = acc + jnp.dot(weight, values, preferred_element_type=jnp.float32)
            whole = totals[1][:, :1] + soft_s[slot, 0, :, :width].astype(jnp.float32)[:, :1]
            carry = carry + jnp.broadcast_to(whole, (rows, width))
        acc_s[...] = acc
        carry_s[...] = carry
        group = entry(2 * at)[0]

        @pl.when(group != entry(2 * at + 2)[0])
        def _():
            for turn_at in range(turns):
                part = acc_s[turn_at * piece : (turn_at + 1) * piece]
                out_ref[group * turns + turn_at] = part.astype(out_ref.dtype)
            acc_s[...] = jnp.zeros_like(acc_s)
            carry_s[...] = jnp.zeros_like(carry_s)

            @pl.when(group + 2 < groups)
            def _():
                arrive(group + 2)

        return 0

    acc_s[...] = jnp.zeros_like(acc_s)
    carry_s[...] = jnp.zeros_like(carry_s)
    lax.fori_loop(0, table_ref.shape[1] // 4 - 1, pair, 0)


def here():
    return lax.axis_index("ep"), lax.rem(lax.axis_index("tp"), 2)


def stick(own, other, blocks, rows, width, turn, turns, spot=here):
    length = own[0].shape[0]
    groups = blocks // turns
    piece = rows // turns
    table = np.array(steps_of(groups, turns), np.int32).reshape(1, -1)
    pairs = 2 * rows * rows * (table.shape[1] // 2 - 2)
    return pl.pallas_call(
        functools.partial(stick_kernel, width**-0.5 * LOG2E, len(own) // 2, turn, turns, spot),
        out_shape=jax.ShapeDtypeStruct((blocks, piece, width), jnp.bfloat16),
        in_specs=[pl.BlockSpec(memory_space=pltpu.SMEM)]
        + [pl.BlockSpec(memory_space=pl.ANY)] * (2 * len(own)),
        out_specs=pl.BlockSpec(memory_space=pltpu.VMEM),
        scratch_shapes=[
            pltpu.VMEM((2, blocks, length, width), jnp.bfloat16),
            pltpu.VMEM((groups + 1, rows, width), jnp.bfloat16),
            pltpu.VMEM((2, blocks, 1, rows), jnp.float32),
            pltpu.VMEM((2 * rows, rows), jnp.bfloat16),
            pltpu.VMEM((rows, rows), jnp.int32),
            pltpu.VMEM((2, 2, rows, rows), jnp.bfloat16),
            pltpu.VMEM((2, 2, rows, rows), jnp.float32),
            pltpu.VMEM((2, rows, rows), jnp.float32),
            pltpu.VMEM((rows, width), jnp.float32),
            pltpu.VMEM((rows, width), jnp.float32),
            pltpu.SemaphoreType.DMA((2, blocks)),
        ],
        cost_estimate=pl.CostEstimate(
            flops=2 * pairs * (rows + 3 * width),
            bytes_accessed=10 * blocks * rows * width,
            transcendentals=3 * pairs,
        ),
    )(jnp.asarray(table), *own, *other)


def project_kernel(back_ref, own_ref, other_ref, first_ref, *rest):
    out_refs, rows_s = rest[:-1], rest[-1]
    tp_index = lax.axis_index("tp")
    core = lax.rem(tp_index, 2)
    heads, _, depth = back_ref.shape
    width = own_ref.shape[0]
    cols = first_ref.shape[1]
    for head in range(heads):
        rows_s[head * depth // width, :, head * depth % width : (head * depth % width) + depth] = back_ref[head]
    own_rows = rows_s[core]
    other_rows = rows_s[1 - core]
    for mask in range(len(out_refs), -1, -1):
        at = pl.ds(pl.multiple_of((tp_index ^ mask) * cols, cols), cols)
        part = jnp.dot(own_rows, own_ref[:, at], preferred_element_type=jnp.float32)
        part += jnp.dot(other_rows, other_ref[:, at], preferred_element_type=jnp.float32)
        ref = out_refs[mask - 1] if mask else first_ref
        ref[...] = part.astype(ref.dtype)


def project(back, own_weight, other_weight, tp_count):
    heads, half, depth = back.shape
    cols = own_weight.shape[1] // tp_count
    vmem = pl.BlockSpec(memory_space=pltpu.VMEM)
    shape = jax.ShapeDtypeStruct((half, cols), jnp.bfloat16)
    return pl.pallas_call(
        project_kernel,
        out_shape=[shape] * tp_count,
        in_specs=[vmem] * 3,
        out_specs=[vmem] * tp_count,
        scratch_shapes=[pltpu.VMEM((2, half, own_weight.shape[0]), jnp.bfloat16)],
        cost_estimate=pl.CostEstimate(
            flops=2 * half * heads * depth * own_weight.shape[1],
            bytes_accessed=4 * own_weight.size + 4 * half * own_weight.shape[1],
            transcendentals=0,
        ),
        compiler_params=pltpu.CompilerParams(vmem_limit_bytes=16 * MIB),
        name="project",
    )(back, own_weight, other_weight)


def finish_kernel(turns, *refs):
    out_ref = refs[-1]
    core = lax.rem(lax.axis_index("tp"), 2)
    piece = refs[0].shape[0]
    count = (len(refs) - 1) // turns
    for turn in range(turns):
        for bit in range(2):
            mine = [ref[...].astype(jnp.float32) for ref in refs[turn * count + bit : (turn + 1) * count : 2]]
            total = functools.reduce(jnp.add, mine)
            part = core if bit == 0 else 1 - core
            at = pl.multiple_of((part * turns + turn) * piece, piece)
            out_ref[pl.ds(at, piece)] = total.astype(out_ref.dtype)


def finish(pieces):
    turns = len(pieces)
    flat = sum(pieces, [])
    rows, cols = flat[0].shape
    vmem = pl.BlockSpec(memory_space=pltpu.VMEM)
    return pl.pallas_call(
        functools.partial(finish_kernel, turns),
        out_shape=jax.ShapeDtypeStruct((2 * turns * rows, cols), jnp.bfloat16),
        in_specs=[vmem] * len(flat),
        out_specs=vmem,
        cost_estimate=pl.CostEstimate(
            flops=8 * rows * turns * cols, bytes_accessed=12 * rows * turns * cols, transcendentals=0
        ),
        compiler_params=pltpu.CompilerParams(vmem_limit_bytes=8 * MIB),
        name="finish",
    )(*flat)


TURNS = 2


def head_attention(messages, out_weight, heads):
    ep_count = lax.axis_size("ep")
    tp_count = lax.axis_size("tp")
    own, other = [], []
    for (k, s), message in zip(rounds_of(heads), messages):
        own.append(send_round(message, heads, k, s))
        other.append(swap(own[-1], "tp", 1))
    depth = out_weight.shape[0] // heads
    half = messages[0].shape[0] // 3 // 16 * 16
    other_weight = swap(out_weight, "tp", 1)
    pieces = []
    for turn in range(TURNS):
        out = stick(own, other, ep_count, half, depth, turn, TURNS)
        back = lax.all_to_all(out, "ep", split_axis=0, concat_axis=0, tiled=True)
        parts = list(project(back, out_weight, other_weight, tp_count))
        for mask in range(1, tp_count):
            parts[mask] = swap(parts[mask], "tp", mask)
        pieces.append(parts)
    return finish(pieces)


def absorb(state, query_heads, piece, visible):
    total, carried = state
    key_piece, value_piece, bias_piece = piece
    span = key_piece.shape[0]
    heads = query_heads.shape[1]
    key_heads = key_piece.reshape(span, heads, -1)
    value_heads = value_piece.reshape(span, heads, -1)
    scale = query_heads.shape[2] ** (-0.5)
    logit = (
        jnp.einsum("qhd,khd->hqk", query_heads, key_heads, preferred_element_type=jnp.float32)
        * scale
    )
    logit = logit + bias_piece.astype(jnp.float32).T[:, None, :]
    keep = jnp.where(visible[None], jax.nn.log_sigmoid(-logit), 0.0)
    stay = lax.cumsum(keep, axis=2, reverse=True) - keep + carried[:, :, None]
    weight = jnp.where(visible[None], jnp.exp(jax.nn.log_sigmoid(logit) + stay), 0.0).astype(
        jnp.bfloat16
    )
    total = total + jnp.einsum(
        "hqk,khd->qhd", weight, value_heads, preferred_element_type=jnp.float32
    )
    return (total, carried + jnp.sum(keep, axis=2))


def fresh_state(query_heads):
    return (
        jnp.zeros(query_heads.shape, jnp.float32),
        jnp.zeros((query_heads.shape[1], query_heads.shape[0]), jnp.float32),
    )


def diagonal(query_heads, piece, offset):
    count = query_heads.shape[0]
    span = piece[0].shape[0]
    key_pos = jnp.arange(span, dtype=jnp.int32)
    query_pos = offset + jnp.arange(count, dtype=jnp.int32)
    visible = key_pos[None, :] < query_pos[:, None]
    return absorb(fresh_state(query_heads), query_heads, piece, visible)


def row_attention(queries, keys, values, key_bias, out_weight):
    span = queries.shape[0]
    heads = key_bias.shape[1]
    query_heads = queries.reshape(span, heads, -1)
    ep_count = lax.axis_size("ep")
    seq_devices = ep_count // SEQUENCE_COUNT
    own_index = lax.axis_index("ep")
    place = own_index % seq_devices
    own_piece = (keys, values, key_bias)
    half = span // 2
    group_bits = seq_devices.bit_length() - 1

    def mirror(rows):
        for bit in range(group_bits):
            rows = partner_2(rows, "ep", bit)
        return rows

    whole = (
        lax.all_gather(own_piece[0], "ep", axis=0, tiled=True),
        lax.all_gather(own_piece[1], "ep", axis=0, tiled=True),
        lax.all_gather(own_piece[2], "ep", axis=0, tiled=True),
    )
    mirror_place = seq_devices - 1 - place
    mirror_index = own_index - place + mirror_place
    early_rows = query_heads[:half]
    late_rows = mirror(queries[half:]).reshape(half, heads, -1)
    partner = tuple(
        (lax.dynamic_slice_in_dim(member, mirror_index * span, span, 0) for member in whole)
    )
    half_visible = jnp.ones((half, span), jnp.bool_)

    def unchanged(inner):
        return inner

    def visit_both(turn, carry):
        early, late = carry
        early_source = jnp.maximum(own_index - turn, 0)
        late_source = jnp.maximum(mirror_index - turn, 0)
        early_piece = tuple(
            (lax.dynamic_slice_in_dim(member, early_source * span, span, 0) for member in whole)
        )
        late_piece = tuple(
            (lax.dynamic_slice_in_dim(member, late_source * span, span, 0) for member in whole)
        )

        def early_taken(inner):
            return absorb(inner, early_rows, early_piece, half_visible)

        def late_taken(inner):
            return absorb(inner, late_rows, late_piece, half_visible)

        early = lax.cond(place >= turn, early_taken, unchanged, early)
        late = lax.cond(mirror_place >= turn, late_taken, unchanged, late)
        return (early, late)

    early_state, late_state = lax.fori_loop(
        1,
        seq_devices,
        visit_both,
        (diagonal(early_rows, own_piece, 0), diagonal(late_rows, partner, half)),
    )
    early_out = early_state[0].astype(jnp.bfloat16).reshape(half, -1)
    late_out = mirror(late_state[0].astype(jnp.bfloat16).reshape(half, -1))
    heads_out = jnp.concatenate([early_out, late_out], axis=0)
    summed = lax.psum_scatter(
        jnp.dot(heads_out, out_weight, preferred_element_type=jnp.float32).astype(jnp.bfloat16),
        "tp",
        scatter_dimension=1,
        tiled=True,
    )
    return summed


def gather_columns(piece):
    count = lax.axis_size("tp")
    index = lax.axis_index("tp")
    cols = piece.shape[1]
    whole = jnp.zeros((piece.shape[0], count * cols), piece.dtype)
    held = [(0, piece)]
    for bit in reversed(range(count.bit_length() - 1)):
        held = held + [(mask | 1 << bit, swap(part, "tp", 1 << bit)) for mask, part in held]
    for mask, part in held:
        whole = lax.dynamic_update_slice(whole, part, (0, (index ^ mask) * cols))
    return whole


def scatter_sum(partial):
    count = lax.axis_size("tp")
    index = lax.axis_index("tp")
    rows = partial.shape[0]
    parts = partial.reshape(rows, count, -1)
    for bit in range(count.bit_length() - 1):
        mine = index >> bit & 1
        parts = parts.reshape(rows, parts.shape[1] // 2, 2, parts.shape[2])
        kept = lax.dynamic_index_in_dim(parts, mine, 2, False)
        sent = lax.dynamic_index_in_dim(parts, 1 - mine, 2, False)
        parts = kept.astype(jnp.float32) + swap(sent.astype(jnp.bfloat16), "tp", 1 << bit)
    return parts.reshape(rows, -1)


def expert_layer(
    moe_input,
    moe_gain,
    route_ids,
    route_scores,
    shared_gate,
    shared_up,
    shared_down,
    expert_gate,
    expert_up,
    expert_down,
):
    ep_count = lax.axis_size("ep")
    token_count, width = moe_input.shape
    cols = width // lax.axis_size("tp")
    inputs = moe_input.astype(jnp.float32)
    normed = (
        inputs * lax.rsqrt(jnp.mean(inputs * inputs, axis=-1, keepdims=True) + EPS_NORM) * moe_gain
    ).astype(jnp.bfloat16)
    own_cols = lax.dynamic_slice_in_dim(normed, lax.axis_index("tp") * cols, cols, 1)
    local_experts = expert_gate.shape[0]
    expert_count = local_experts * ep_count
    topk = route_ids.shape[1]
    capacity = 3 * token_count * topk // (2 * expert_count)
    slots = expert_count * capacity
    pairs = token_count * topk
    chosen = route_ids.reshape(-1)
    pair_at = jnp.arange(pairs, dtype=jnp.int32)
    earlier = (chosen[:, None] == chosen[None, :]) & (pair_at[None, :] < pair_at[:, None])
    place_in = jnp.sum(earlier.astype(jnp.int32), axis=1)
    slot_ids = (chosen * capacity + place_in).reshape(token_count, topk)
    slot_at = jnp.arange(slots, dtype=jnp.int32)
    picks = [(slot_ids[:, k, None] == slot_at[None, :]) for k in range(topk)]
    dispatch = functools.reduce(jnp.logical_or, picks).astype(jnp.bfloat16)
    outgoing = lax.dot_general(
        dispatch, own_cols, (((0,), (0,)), ((), ())), preferred_element_type=jnp.float32
    ).astype(jnp.bfloat16)
    arrived = lax.all_to_all(outgoing, "ep", split_axis=0, concat_axis=0, tiled=True)
    piece = gather_columns(arrived)
    shared_hidden = (
        jax.nn.silu(jnp.dot(normed, shared_gate, preferred_element_type=jnp.float32))
        * jnp.dot(normed, shared_up, preferred_element_type=jnp.float32)
    ).astype(jnp.bfloat16)
    common = jnp.dot(shared_hidden, shared_down, preferred_element_type=jnp.float32)
    if local_experts == 1:
        grid = piece
        gate_sum = jnp.dot(grid, expert_gate[0], preferred_element_type=jnp.float32)
        up_sum = jnp.dot(grid, expert_up[0], preferred_element_type=jnp.float32)
        expert_hidden = (jax.nn.silu(gate_sum) * up_sum).astype(jnp.bfloat16)
        routed = jnp.dot(expert_hidden, expert_down[0], preferred_element_type=jnp.float32)
    else:
        grid = piece.reshape(ep_count, local_experts, capacity, width)
        gate_sum = jnp.einsum("secd,edf->secf", grid, expert_gate, preferred_element_type=jnp.float32)
        up_sum = jnp.einsum("secd,edf->secf", grid, expert_up, preferred_element_type=jnp.float32)
        expert_hidden = (jax.nn.silu(gate_sum) * up_sum).astype(jnp.bfloat16)
        routed = jnp.einsum(
            "secf,efd->secd", expert_hidden, expert_down, preferred_element_type=jnp.float32
        ).reshape(slots, width)
    summed = scatter_sum(jnp.concatenate([routed, common], axis=0).astype(jnp.bfloat16))
    returned = lax.all_to_all(
        summed[:slots].astype(jnp.bfloat16), "ep", split_axis=0, concat_axis=0, tiled=True
    )
    gates = route_scores / jnp.sum(route_scores, axis=-1, keepdims=True) * ROUTED_SCALE
    mix = summed[slots:]
    for k in range(topk):
        row = jnp.dot(picks[k].astype(jnp.bfloat16), returned, preferred_element_type=jnp.float32)
        mix = mix + row * gates[:, k, None]
    return mix.astype(jnp.bfloat16)


def gather_pieces(piece):
    pieces = [piece]
    for mask in range(1, lax.axis_size("tp")):
        pieces.append(swap(piece, "tp", mask))
    return pieces


def scatter_rest(kept, sent):
    index = lax.axis_index("tp")
    parts = kept.astype(jnp.float32) + swap(sent, "tp", 1)
    for bit in range(1, lax.axis_size("tp").bit_length() - 1):
        mine = index >> bit & 1
        parts = parts.reshape(parts.shape[0] // 2, 2, *parts.shape[1:])
        stay = lax.dynamic_index_in_dim(parts, mine, 1, False)
        leave = lax.dynamic_index_in_dim(parts, 1 - mine, 1, False)
        parts = stay + swap(leave.astype(jnp.bfloat16), "tp", 1 << bit)
    return parts[0]


def route_kernel(capacity, input_ref, gain_ref, ids_ref, out_ref, normed_ref, slots_ref):
    tokens, _ = input_ref.shape
    slots, cols = out_ref.shape
    topk = ids_ref.shape[0]
    inputs = input_ref[...].astype(jnp.float32)
    mean = jnp.mean(inputs * inputs, axis=-1, keepdims=True)
    normed_ref[...] = (inputs * lax.rsqrt(mean + EPS_NORM) * gain_ref[...]).astype(jnp.bfloat16)
    experts_at = -(-(slots // capacity) // 16) * 16
    expert = lax.broadcasted_iota(jnp.int32, (experts_at, tokens), 0)
    named = [ids_ref[k : k + 1] == expert for k in range(topk)]
    count = functools.reduce(jnp.add, [jnp.where(n, 1.0, 0.0) for n in named]).astype(jnp.bfloat16)
    row = lax.broadcasted_iota(jnp.int32, (tokens, tokens), 0)
    column = lax.broadcasted_iota(jnp.int32, (tokens, tokens), 1)
    before = jnp.where(row < column, 1.0, 0.0).astype(jnp.bfloat16)
    earlier = jnp.dot(count, before, preferred_element_type=jnp.float32)
    slot_at = lax.broadcasted_iota(jnp.int32, (slots, tokens), 0)
    taken = None
    for k in range(topk):
        place = jnp.sum(jnp.where(named[k], earlier, 0.0), axis=0, keepdims=True)
        slot = ids_ref[k : k + 1] * capacity + place.astype(jnp.int32)
        slots_ref[k : k + 1] = slot
        taken = slot_at == slot if taken is None else taken | (slot_at == slot)
    own = normed_ref[:, pl.ds(pl.multiple_of(lax.axis_index("tp") * cols, cols), cols)]
    out_ref[...] = jnp.dot(
        jnp.where(taken, 1.0, 0.0).astype(jnp.bfloat16), own, preferred_element_type=jnp.float32
    ).astype(out_ref.dtype)


def route(moe_input, moe_gain, route_ids, capacity, slots, cols):
    tokens, width = moe_input.shape
    vmem = pl.BlockSpec(memory_space=pltpu.VMEM)
    return pl.pallas_call(
        functools.partial(route_kernel, capacity),
        out_shape=[
            jax.ShapeDtypeStruct((slots, cols), jnp.bfloat16),
            jax.ShapeDtypeStruct((tokens, width), jnp.bfloat16),
            jax.ShapeDtypeStruct(route_ids.shape, jnp.int32),
        ],
        in_specs=[vmem] * 3,
        out_specs=[vmem] * 3,
        cost_estimate=pl.CostEstimate(
            flops=2 * slots * tokens * cols, bytes_accessed=6 * moe_input.size, transcendentals=tokens
        ),
        name="route",
    )(moe_input, moe_gain.reshape(1, width), route_ids)


def silu_product(gate_sum, up_sum):
    return (gate_sum / (1.0 + jnp.exp(-gate_sum)) * up_sum).astype(jnp.bfloat16)


def experts_kernel(shared_ref, shared_down_ref, gate_ref, up_ref, down_ref, *refs):
    pieces, (kept_ref, sent_ref) = refs[:-2], refs[-2:]
    tp_index = lax.axis_index("tp")
    core = lax.rem(tp_index, 2)
    slots, cols = pieces[0].shape
    gate_sum = up_sum = None
    for mask, piece in enumerate(pieces):
        at = pl.ds(pl.multiple_of((tp_index ^ mask) * cols, cols), cols)
        gate = jnp.dot(piece[...], gate_ref[0, at], preferred_element_type=jnp.float32)
        up = jnp.dot(piece[...], up_ref[0, at], preferred_element_type=jnp.float32)
        gate_sum = gate if gate_sum is None else gate_sum + gate
        up_sum = up if up_sum is None else up_sum + up
    hidden = silu_product(gate_sum, up_sum)
    for far in range(kept_ref.shape[0]):
        for ref, near in ((kept_ref, core), (sent_ref, 1 - core)):
            at = pl.ds(pl.multiple_of((2 * far + near) * cols, cols), cols)
            ref[far, :slots] = jnp.dot(
                hidden, down_ref[0, :, at], preferred_element_type=jnp.float32
            ).astype(ref.dtype)
            ref[far, slots:] = jnp.dot(
                shared_ref[...], shared_down_ref[:, at], preferred_element_type=jnp.float32
            ).astype(ref.dtype)


def experts(shared_hidden, shared_down, gate, up, down, pieces):
    slots, cols = pieces[0].shape
    rows = slots + shared_hidden.shape[0]
    vmem = pl.BlockSpec(memory_space=pltpu.VMEM)
    shape = jax.ShapeDtypeStruct((len(pieces) // 2, rows, cols), jnp.bfloat16)
    return pl.pallas_call(
        experts_kernel,
        out_shape=[shape, shape],
        in_specs=[vmem] * (5 + len(pieces)),
        out_specs=[vmem, vmem],
        cost_estimate=pl.CostEstimate(
            flops=6 * slots * gate.size + 2 * shared_hidden.size * shared_down.shape[1],
            bytes_accessed=2 * (3 * gate.size + shared_down.size + 2 * rows * cols * len(pieces)),
            transcendentals=slots * gate.shape[2],
        ),
        compiler_params=pltpu.CompilerParams(vmem_limit_bytes=30 * MIB),
        name="experts",
    )(shared_hidden, shared_down, gate, up, down, *pieces)


def combine_kernel(common_ref, returned_ref, slots_ref, scores_ref, out_ref):
    scores = scores_ref[...]
    gates = scores / jnp.sum(scores, axis=0, keepdims=True) * ROUTED_SCALE
    tokens = out_ref.shape[0]
    slot_at = lax.broadcasted_iota(jnp.int32, (returned_ref.shape[0], tokens), 0)
    share = jnp.zeros(slot_at.shape, jnp.float32)
    for k in range(scores.shape[0]):
        share = share + jnp.where(slot_at == slots_ref[k : k + 1], gates[k : k + 1], 0.0)
    high = share.astype(jnp.bfloat16)
    low = (share - high.astype(jnp.float32)).astype(jnp.bfloat16)
    mix = common_ref[...]
    for part in (high, low):
        mix = mix + lax.dot_general(
            part, returned_ref[...], (((0,), (0,)), ((), ())), preferred_element_type=jnp.float32
        )
    out_ref[...] = mix.astype(out_ref.dtype)


def combine(common, returned, slot_ids, route_scores):
    vmem = pl.BlockSpec(memory_space=pltpu.VMEM)
    return pl.pallas_call(
        combine_kernel,
        out_shape=jax.ShapeDtypeStruct(common.shape, jnp.bfloat16),
        in_specs=[vmem] * 4,
        out_specs=vmem,
        cost_estimate=pl.CostEstimate(
            flops=4 * common.size * returned.shape[0],
            bytes_accessed=6 * common.size + 2 * returned.size,
            transcendentals=0,
        ),
        compiler_params=pltpu.CompilerParams(vmem_limit_bytes=8 * MIB),
        name="combine",
    )(common, returned, slot_ids, route_scores)


def expert_layer_near(
    moe_input,
    moe_gain,
    route_ids,
    route_scores,
    shared_gate,
    shared_up,
    shared_down,
    expert_gate,
    expert_up,
    expert_down,
):
    ep_count = lax.axis_size("ep")
    token_count, width = moe_input.shape
    cols = width // lax.axis_size("tp")
    expert_count = expert_gate.shape[0] * ep_count
    capacity = 3 * token_count * route_ids.shape[1] // (2 * expert_count)
    slots = expert_count * capacity
    outgoing, normed, slot_ids = route(
        moe_input, moe_gain, route_ids.T, capacity, slots, cols
    )
    arrived = lax.all_to_all(outgoing, "ep", split_axis=0, concat_axis=0, tiled=True)
    pieces = gather_pieces(arrived)
    shared_hidden = silu_product(
        jnp.dot(normed, shared_gate, preferred_element_type=jnp.float32),
        jnp.dot(normed, shared_up, preferred_element_type=jnp.float32),
    )
    kept, sent = experts(
        shared_hidden, shared_down, expert_gate, expert_up, expert_down, pieces
    )
    summed = scatter_rest(kept, sent)
    returned = lax.all_to_all(
        summed[:slots].astype(jnp.bfloat16), "ep", split_axis=0, concat_axis=0, tiled=True
    )
    return combine(summed[slots:], returned, slot_ids, route_scores.T)


def body(queries, keys, values, key_bias, out_weight, *moe):
    ep_count, tp_count = lax.axis_size("ep"), lax.axis_size("tp")
    span, width = queries.shape
    heads = key_bias.shape[1]
    cols = out_weight.shape[1] // tp_count
    tokens = moe[0].shape[0]
    slots = 3 * tokens * moe[2].shape[1] // 2
    aligned = span % 512 == 0 and width % (128 * heads) == 0 and cols % 256 == 0 and slots % 16 == 0
    near = SEQUENCE_COUNT == 1 and 2 * heads == ep_count and tp_count % 2 == 0 and aligned
    if not near or moe[7].shape[0] != 1 or slots % ep_count or tokens % 128:
        return (
            row_attention(queries, keys, values, key_bias, out_weight),
            expert_layer(*moe),
        )
    messages = pack(keys, values, queries, key_bias.T)
    mixed = head_attention(messages, out_weight, heads)
    return (mixed, expert_layer_near(*moe))


def solution(mesh):
    return jax.shard_map(
        body,
        mesh=mesh,
        in_specs=(
            P("ep", "tp"),
            P("ep", "tp"),
            P("ep", "tp"),
            P("ep", "tp"),
            P("tp", None),
            P("ep", None),
            P(),
            P("ep", None),
            P("ep", None),
            P(None, "tp"),
            P(None, "tp"),
            P("tp", None),
            P("ep", None, "tp"),
            P("ep", None, "tp"),
            P("ep", "tp", None),
        ),
        out_specs=(P("ep", "tp"), P("ep", "tp")),
        check_vma=False,
    )
```

```python
import functools

import jax
import jax.numpy as jnp
import numpy as np
from jax import lax
from jax.experimental import pallas as pl
from jax.experimental.pallas import tpu as pltpu
from jax.sharding import PartitionSpec as P


SEQUENCE_COUNT = 1


EPS_NORM = 1e-06
ROUTED_SCALE = 2.5
LOG2E = 1.4426950408889634
NEVER = -1e30
MIB = 1 << 20


def partner_2(array, axis, apart):
    return lax.ppermute(array, axis, [(i, i ^ 1 << apart) for i in range(lax.axis_size(axis))])


def swap(array, axis, mask):
    return lax.ppermute(array, axis, [(i, i ^ mask) for i in range(lax.axis_size(axis))])


def rounds_of(heads):
    return [(k, s) for k in range(heads) for s in range(2)]


def send_round(array, heads, k, s):
    ep_count, tp_count = lax.axis_size("ep"), lax.axis_size("tp")
    pairs = []
    for i in range(ep_count):
        for t in range(tp_count):
            core = t % 2
            to_ep = core * heads + (i + k) % heads
            to_tp = t - core + (i // heads + s) % 2
            pairs.append((i * tp_count + t, to_ep * tp_count + to_tp))
    return lax.ppermute(array, ("ep", "tp"), pairs)


def pack_kernel(heads, k_ref, v_ref, q_ref, bias_ref, *refs):
    out_refs, bias_s = refs[:-1], refs[-1]
    own = lax.axis_index("ep")
    span = k_ref.shape[0]
    half = span // 2
    depth = k_ref.shape[1] // heads
    bias_rows = half // depth
    turned = bias_ref[...].astype(jnp.float32)
    for head in range(heads):
        for r in range(span // depth):
            bias_s[head, r] = turned[head : head + 1, r * depth : (r + 1) * depth]
    for (k, s), out_ref in zip(rounds_of(heads), out_refs):
        head = lax.rem(own + k, heads)
        part = lax.rem(own // heads + s, 2)
        rows = pl.ds(pl.multiple_of(part * half, half), half)
        lanes = pl.ds(pl.multiple_of(head * depth, depth), depth)
        out_ref[:half] = k_ref[rows, lanes]
        out_ref[half : 2 * half] = v_ref[rows, lanes]
        pad = out_ref.shape[0] - 3 * half
        at = lax.broadcasted_iota(jnp.int32, (pad, depth), 0)
        bias = jnp.zeros((pad, depth), jnp.float32)
        for r in range(bias_rows):
            bias = jnp.where(at == r, bias_s[head, part * bias_rows + r], bias)
        out_ref[2 * half : 2 * half + pad] = bias.astype(out_ref.dtype)
        out_ref[2 * half + pad :] = q_ref[rows, lanes]


def pack(keys, values, queries, bias):
    heads, span = bias.shape
    half, depth = span // 2, keys.shape[1] // heads
    pad = -(-(half // depth) // 16) * 16
    vmem = pl.BlockSpec(memory_space=pltpu.VMEM)
    count = len(rounds_of(heads))
    shape = jax.ShapeDtypeStruct((3 * half + pad, depth), keys.dtype)
    return pl.pallas_call(
        functools.partial(pack_kernel, heads),
        out_shape=[shape] * count,
        in_specs=[vmem] * 4,
        out_specs=[vmem] * count,
        scratch_shapes=[pltpu.VMEM((heads, span // depth, 1, depth), jnp.float32)],
        cost_estimate=pl.CostEstimate(
            flops=keys.size * 8, bytes_accessed=12 * keys.size, transcendentals=0
        ),
        name="pack",
    )(keys, values, queries, bias)


def steps_of(blocks):
    steps = [(block, source) for block in range(blocks) for source in reversed(range(block + 1))]
    return steps + [(blocks, 0)] * (2 + len(steps) % 2)


def stick_kernel(scale, heads, turns, spot, table_ref, *refs):
    count = 2 * heads
    messages, out_refs = refs[: 2 * count], refs[2 * count : 2 * count + turns]
    mes_s, q_s, b_s, tri_s, reach_s, soft_s, log_s, prod_s, acc_s, carry_s, sems = refs[
        2 * count + turns :
    ]
    _, blocks, length, width = mes_s.shape
    rows = turns * out_refs[0].shape[1]
    bias_rows = rows // width
    pad = length - 3 * rows
    place, mine = spot()
    for at, which in enumerate((mine, 1 - mine)):
        for (k, s), ref in zip(rounds_of(heads), messages[at * count : (at + 1) * count]):
            block = lax.rem(which + s, 2) * heads + lax.rem(place + heads - k, heads)
            pltpu.make_async_copy(ref, mes_s.at[which, block], sems.at[which, block]).start()
    later = lax.broadcasted_iota(jnp.int32, (2 * rows, rows), 0)
    column = lax.broadcasted_iota(jnp.int32, (2 * rows, rows), 1)
    tri_s[...] = jnp.where(later > column, 1.0, 0.0).astype(jnp.bfloat16)
    row = lax.broadcasted_iota(jnp.int32, (rows, rows), 0)
    reach_s[...] = lax.broadcasted_iota(jnp.int32, (rows, rows), 1) - row - mine * rows
    for block in range(blocks):
        for which in (0, 1):
            pltpu.make_async_copy(messages[0], mes_s.at[which, block], sems.at[which, block]).wait()
            lanes = [
                mes_s[which, block, 2 * rows + r : 2 * rows + r + 1, :].astype(jnp.float32)
                for r in range(bias_rows)
            ]
            b_s[which, block] = jnp.concatenate(lanes, axis=1) * LOG2E
        q_s[block] = mes_s[mine, block, 2 * rows + pad :]
    q_s[blocks] = q_s[0]
    parts = (1, 0)

    def scores(block, source):
        return [
            lax.dot_general(
                q_s[block],
                mes_s[part, source, :rows],
                (((1,), (1,)), ((), ())),
                preferred_element_type=jnp.float32,
            )
            for part in parts
        ]

    def soften(slot, block, source):
        ahead = (block - source) * (2 * rows)
        for part in parts:
            logit = prod_s[part] * scale + b_s[part, source]
            logit = jnp.where(reach_s[...] < ahead - part * rows, logit, NEVER)
            soft = jnp.maximum(logit, jnp.log2(1.0 + jnp.exp2(jnp.minimum(logit, 64.0))))
            soft_s[slot, part] = soft.astype(jnp.bfloat16)
            log_s[slot, part] = logit - soft

    def sums(slot):
        one = jnp.dot(soft_s[slot, 1], tri_s[:rows], preferred_element_type=jnp.float32)
        both = jnp.concatenate([soft_s[slot, 0], soft_s[slot, 1]], axis=1)
        return [one, jnp.dot(both, tri_s[...], preferred_element_type=jnp.float32)]

    def entry(t):
        return table_ref[0, 2 * t], table_ref[0, 2 * t + 1]

    def put(products):
        for part, product in zip(parts, products):
            prod_s[part] = product

    put(scores(*entry(0)))
    soften(0, *entry(0))
    put(scores(*entry(1)))

    def pair(at, _):
        acc = acc_s[...]
        carry = carry_s[...]
        for slot in range(2):
            t = 2 * at + slot
            soften(1 - slot, *entry(t + 1))
            products = scores(*entry(t + 2))
            totals = sums(slot)
            put(products)
            wide = jnp.concatenate([carry] * bias_rows, axis=1)
            block, source = entry(t)
            for part, total in zip(parts, totals):
                weight = jnp.exp2(log_s[slot, part] - (total + wide)).astype(jnp.bfloat16)
                values = mes_s[part, source, rows : 2 * rows]
                acc = acc + jnp.dot(weight, values, preferred_element_type=jnp.float32)
            whole = totals[1][:, :1] + soft_s[slot, 0, :, :width].astype(jnp.float32)[:, :1]
            carry = carry + jnp.broadcast_to(whole, (rows, width))
            for turn, out_ref in enumerate(out_refs):
                piece = out_ref.shape[1]
                out_ref[block] = acc[turn * piece : (turn + 1) * piece].astype(out_ref.dtype)
            more = source > 0
            acc = jnp.where(more, acc, 0.0)
            carry = jnp.where(more, carry, 0.0)
        acc_s[...] = acc
        carry_s[...] = carry
        return 0

    acc_s[...] = jnp.zeros_like(acc_s)
    carry_s[...] = jnp.zeros_like(carry_s)
    pairs = table_ref.shape[1] // 4 - 1
    unroll = max(u for u in range(1, 10) if pairs % u == 0)
    lax.fori_loop(0, pairs, pair, 0, unroll=unroll)


def here():
    return lax.axis_index("ep"), lax.rem(lax.axis_index("tp"), 2)


def stick(own, other, blocks, rows, width, turns, spot=here):
    length = own[0].shape[0]
    table = np.array(steps_of(blocks), np.int32).reshape(1, -1)
    pairs = 2 * rows * rows * (table.shape[1] // 2 - 2)
    shape = jax.ShapeDtypeStruct((blocks, rows // turns, width), jnp.bfloat16)
    return pl.pallas_call(
        functools.partial(stick_kernel, width**-0.5 * LOG2E, len(own) // 2, turns, spot),
        out_shape=[shape] * turns,
        in_specs=[pl.BlockSpec(memory_space=pltpu.SMEM)]
        + [pl.BlockSpec(memory_space=pl.ANY)] * (2 * len(own)),
        out_specs=[pl.BlockSpec(memory_space=pltpu.VMEM)] * turns,
        scratch_shapes=[
            pltpu.VMEM((2, blocks, length, width), jnp.bfloat16),
            pltpu.VMEM((blocks + 1, rows, width), jnp.bfloat16),
            pltpu.VMEM((2, blocks, 1, rows), jnp.float32),
            pltpu.VMEM((2 * rows, rows), jnp.bfloat16),
            pltpu.VMEM((rows, rows), jnp.int32),
            pltpu.VMEM((2, 2, rows, rows), jnp.bfloat16),
            pltpu.VMEM((2, 2, rows, rows), jnp.float32),
            pltpu.VMEM((2, rows, rows), jnp.float32),
            pltpu.VMEM((rows, width), jnp.float32),
            pltpu.VMEM((rows, width), jnp.float32),
            pltpu.SemaphoreType.DMA((2, blocks)),
        ],
        cost_estimate=pl.CostEstimate(
            flops=2 * pairs * (rows + 3 * width),
            bytes_accessed=10 * blocks * rows * width,
            transcendentals=3 * pairs,
        ),
        name="stick",
    )(jnp.asarray(table), *own, *other)


def project_kernel(masks, own_ref, other_ref, *refs):
    count = len(masks)
    back_refs, out_refs, rows_s = refs[: -count - 1], refs[-count - 1 : -1], refs[-1]
    ep_index, tp_index = lax.axis_index("ep"), lax.axis_index("tp")
    core = lax.rem(tp_index, 2)
    width = own_ref.shape[0]
    cols = out_refs[0].shape[1]
    depth = back_refs[0].shape[-1]
    heads = rows_s.shape[1] // depth
    for head in range(heads):
        if len(back_refs) == 1:
            rows_s[:, head * depth : (head + 1) * depth] = back_refs[0][head]
        else:
            at = pl.ds(pl.multiple_of((ep_index ^ head) * depth, depth), depth)
            ref = back_refs[head]
            rows_s[:, at] = ref[...] if head else ref[ep_index]
    own_rows = rows_s[:, pl.ds(pl.multiple_of(core * width, width), width)]
    other_rows = rows_s[:, pl.ds(pl.multiple_of((1 - core) * width, width), width)]
    for mask, out_ref in zip(masks, out_refs):
        at = pl.ds(pl.multiple_of((tp_index ^ mask) * cols, cols), cols)
        part = jnp.dot(own_rows, own_ref[:, at], preferred_element_type=jnp.float32)
        part += jnp.dot(other_rows, other_ref[:, at], preferred_element_type=jnp.float32)
        out_ref[...] = part.astype(out_ref.dtype)


def project(back, own_weight, other_weight, tp_count, masks):
    rows = back[0].shape[1]
    cols = own_weight.shape[1] // tp_count
    vmem = pl.BlockSpec(memory_space=pltpu.VMEM)
    shape = jax.ShapeDtypeStruct((rows, cols), jnp.bfloat16)
    return pl.pallas_call(
        functools.partial(project_kernel, masks),
        out_shape=[shape] * len(masks),
        in_specs=[vmem] * (2 + len(back)),
        out_specs=[vmem] * len(masks),
        scratch_shapes=[pltpu.VMEM((rows, 2 * own_weight.shape[0]), jnp.bfloat16)],
        cost_estimate=pl.CostEstimate(
            flops=4 * rows * own_weight.size * len(masks) // tp_count,
            bytes_accessed=4 * own_weight.size + 4 * rows * own_weight.shape[1],
            transcendentals=0,
        ),
        compiler_params=pltpu.CompilerParams(vmem_limit_bytes=16 * MIB),
        name="project",
    )(own_weight, other_weight, *back)


def finish_kernel(turns, *refs):
    out_ref = refs[-1]
    core = lax.rem(lax.axis_index("tp"), 2)
    piece = refs[0].shape[0]
    count = (len(refs) - 1) // turns
    for turn in range(turns):
        for bit in range(2):
            mine = [ref[...].astype(jnp.float32) for ref in refs[turn * count + bit : (turn + 1) * count : 2]]
            total = functools.reduce(jnp.add, mine)
            part = core if bit == 0 else 1 - core
            at = pl.multiple_of((part * turns + turn) * piece, piece)
            out_ref[pl.ds(at, piece)] = total.astype(out_ref.dtype)


def finish(pieces):
    turns = len(pieces)
    flat = sum(pieces, [])
    rows, cols = flat[0].shape
    vmem = pl.BlockSpec(memory_space=pltpu.VMEM)
    return pl.pallas_call(
        functools.partial(finish_kernel, turns),
        out_shape=jax.ShapeDtypeStruct((2 * turns * rows, cols), jnp.bfloat16),
        in_specs=[vmem] * len(flat),
        out_specs=vmem,
        cost_estimate=pl.CostEstimate(
            flops=8 * rows * turns * cols, bytes_accessed=12 * rows * turns * cols, transcendentals=0
        ),
        compiler_params=pltpu.CompilerParams(vmem_limit_bytes=8 * MIB),
        name="finish",
    )(*flat)


TURNS = 1


def head_attention(messages, out_weight, heads):
    ep_count = lax.axis_size("ep")
    tp_count = lax.axis_size("tp")
    own, other = [], []
    for (k, s), message in zip(rounds_of(heads), messages):
        own.append(send_round(message, heads, k, s))
        other.append(swap(own[-1], "tp", 1))
    depth = out_weight.shape[0] // heads
    half = messages[0].shape[0] // 3 // 16 * 16
    other_weight = swap(out_weight, "tp", 1)
    outs = stick(own, other, ep_count, half, depth, TURNS)
    backs = []
    backs.append([lax.all_to_all(outs[0], "ep", split_axis=0, concat_axis=0, tiled=True)])
    ep_index = lax.axis_index("ep")
    for turn in range(1, TURNS):
        back = [outs[turn]]
        for mask in range(1, ep_count):
            row = lax.dynamic_index_in_dim(outs[turn], ep_index ^ mask, 0, False)
            back.append(swap(row, "ep", mask))
        backs.append(back)
    pieces = []
    for back in backs:
        parts = {}
        for masks in (range(tp_count - 1, 1, -1), (1, 0)):
            made = project(back, out_weight, other_weight, tp_count, tuple(masks))
            for mask, part in zip(masks, made):
                parts[mask] = swap(part, "tp", mask) if mask else part
        pieces.append([parts[mask] for mask in range(tp_count)])
    return finish(pieces)


def absorb(state, query_heads, piece, visible):
    total, carried = state
    key_piece, value_piece, bias_piece = piece
    span = key_piece.shape[0]
    heads = query_heads.shape[1]
    key_heads = key_piece.reshape(span, heads, -1)
    value_heads = value_piece.reshape(span, heads, -1)
    scale = query_heads.shape[2] ** (-0.5)
    logit = (
        jnp.einsum("qhd,khd->hqk", query_heads, key_heads, preferred_element_type=jnp.float32)
        * scale
    )
    logit = logit + bias_piece.astype(jnp.float32).T[:, None, :]
    keep = jnp.where(visible[None], jax.nn.log_sigmoid(-logit), 0.0)
    stay = lax.cumsum(keep, axis=2, reverse=True) - keep + carried[:, :, None]
    weight = jnp.where(visible[None], jnp.exp(jax.nn.log_sigmoid(logit) + stay), 0.0).astype(
        jnp.bfloat16
    )
    total = total + jnp.einsum(
        "hqk,khd->qhd", weight, value_heads, preferred_element_type=jnp.float32
    )
    return (total, carried + jnp.sum(keep, axis=2))


def fresh_state(query_heads):
    return (
        jnp.zeros(query_heads.shape, jnp.float32),
        jnp.zeros((query_heads.shape[1], query_heads.shape[0]), jnp.float32),
    )


def diagonal(query_heads, piece, offset):
    count = query_heads.shape[0]
    span = piece[0].shape[0]
    key_pos = jnp.arange(span, dtype=jnp.int32)
    query_pos = offset + jnp.arange(count, dtype=jnp.int32)
    visible = key_pos[None, :] < query_pos[:, None]
    return absorb(fresh_state(query_heads), query_heads, piece, visible)


def row_attention(queries, keys, values, key_bias, out_weight):
    span = queries.shape[0]
    heads = key_bias.shape[1]
    query_heads = queries.reshape(span, heads, -1)
    ep_count = lax.axis_size("ep")
    seq_devices = ep_count // SEQUENCE_COUNT
    own_index = lax.axis_index("ep")
    place = own_index % seq_devices
    own_piece = (keys, values, key_bias)
    half = span // 2
    group_bits = seq_devices.bit_length() - 1

    def mirror(rows):
        for bit in range(group_bits):
            rows = partner_2(rows, "ep", bit)
        return rows

    whole = (
        lax.all_gather(own_piece[0], "ep", axis=0, tiled=True),
        lax.all_gather(own_piece[1], "ep", axis=0, tiled=True),
        lax.all_gather(own_piece[2], "ep", axis=0, tiled=True),
    )
    mirror_place = seq_devices - 1 - place
    mirror_index = own_index - place + mirror_place
    early_rows = query_heads[:half]
    late_rows = mirror(queries[half:]).reshape(half, heads, -1)
    partner = tuple(
        (lax.dynamic_slice_in_dim(member, mirror_index * span, span, 0) for member in whole)
    )
    half_visible = jnp.ones((half, span), jnp.bool_)

    def unchanged(inner):
        return inner

    def visit_both(turn, carry):
        early, late = carry
        early_source = jnp.maximum(own_index - turn, 0)
        late_source = jnp.maximum(mirror_index - turn, 0)
        early_piece = tuple(
            (lax.dynamic_slice_in_dim(member, early_source * span, span, 0) for member in whole)
        )
        late_piece = tuple(
            (lax.dynamic_slice_in_dim(member, late_source * span, span, 0) for member in whole)
        )

        def early_taken(inner):
            return absorb(inner, early_rows, early_piece, half_visible)

        def late_taken(inner):
            return absorb(inner, late_rows, late_piece, half_visible)

        early = lax.cond(place >= turn, early_taken, unchanged, early)
        late = lax.cond(mirror_place >= turn, late_taken, unchanged, late)
        return (early, late)

    early_state, late_state = lax.fori_loop(
        1,
        seq_devices,
        visit_both,
        (diagonal(early_rows, own_piece, 0), diagonal(late_rows, partner, half)),
    )
    early_out = early_state[0].astype(jnp.bfloat16).reshape(half, -1)
    late_out = mirror(late_state[0].astype(jnp.bfloat16).reshape(half, -1))
    heads_out = jnp.concatenate([early_out, late_out], axis=0)
    summed = lax.psum_scatter(
        jnp.dot(heads_out, out_weight, preferred_element_type=jnp.float32).astype(jnp.bfloat16),
        "tp",
        scatter_dimension=1,
        tiled=True,
    )
    return summed


def gather_columns(piece):
    count = lax.axis_size("tp")
    index = lax.axis_index("tp")
    cols = piece.shape[1]
    whole = jnp.zeros((piece.shape[0], count * cols), piece.dtype)
    held = [(0, piece)]
    for bit in reversed(range(count.bit_length() - 1)):
        held = held + [(mask | 1 << bit, swap(part, "tp", 1 << bit)) for mask, part in held]
    for mask, part in held:
        whole = lax.dynamic_update_slice(whole, part, (0, (index ^ mask) * cols))
    return whole


def scatter_sum(partial):
    count = lax.axis_size("tp")
    index = lax.axis_index("tp")
    rows = partial.shape[0]
    parts = partial.reshape(rows, count, -1)
    for bit in range(count.bit_length() - 1):
        mine = index >> bit & 1
        parts = parts.reshape(rows, parts.shape[1] // 2, 2, parts.shape[2])
        kept = lax.dynamic_index_in_dim(parts, mine, 2, False)
        sent = lax.dynamic_index_in_dim(parts, 1 - mine, 2, False)
        parts = kept.astype(jnp.float32) + swap(sent.astype(jnp.bfloat16), "tp", 1 << bit)
    return parts.reshape(rows, -1)


def expert_layer(
    moe_input,
    moe_gain,
    route_ids,
    route_scores,
    shared_gate,
    shared_up,
    shared_down,
    expert_gate,
    expert_up,
    expert_down,
):
    ep_count = lax.axis_size("ep")
    token_count, width = moe_input.shape
    cols = width // lax.axis_size("tp")
    inputs = moe_input.astype(jnp.float32)
    normed = (
        inputs * lax.rsqrt(jnp.mean(inputs * inputs, axis=-1, keepdims=True) + EPS_NORM) * moe_gain
    ).astype(jnp.bfloat16)
    own_cols = lax.dynamic_slice_in_dim(normed, lax.axis_index("tp") * cols, cols, 1)
    local_experts = expert_gate.shape[0]
    expert_count = local_experts * ep_count
    topk = route_ids.shape[1]
    capacity = 3 * token_count * topk // (2 * expert_count)
    slots = expert_count * capacity
    pairs = token_count * topk
    chosen = route_ids.reshape(-1)
    pair_at = jnp.arange(pairs, dtype=jnp.int32)
    earlier = (chosen[:, None] == chosen[None, :]) & (pair_at[None, :] < pair_at[:, None])
    place_in = jnp.sum(earlier.astype(jnp.int32), axis=1)
    slot_ids = (chosen * capacity + place_in).reshape(token_count, topk)
    slot_at = jnp.arange(slots, dtype=jnp.int32)
    picks = [(slot_ids[:, k, None] == slot_at[None, :]) for k in range(topk)]
    dispatch = functools.reduce(jnp.logical_or, picks).astype(jnp.bfloat16)
    outgoing = lax.dot_general(
        dispatch, own_cols, (((0,), (0,)), ((), ())), preferred_element_type=jnp.float32
    ).astype(jnp.bfloat16)
    arrived = lax.all_to_all(outgoing, "ep", split_axis=0, concat_axis=0, tiled=True)
    piece = gather_columns(arrived)
    shared_hidden = (
        jax.nn.silu(jnp.dot(normed, shared_gate, preferred_element_type=jnp.float32))
        * jnp.dot(normed, shared_up, preferred_element_type=jnp.float32)
    ).astype(jnp.bfloat16)
    common = jnp.dot(shared_hidden, shared_down, preferred_element_type=jnp.float32)
    if local_experts == 1:
        grid = piece
        gate_sum = jnp.dot(grid, expert_gate[0], preferred_element_type=jnp.float32)
        up_sum = jnp.dot(grid, expert_up[0], preferred_element_type=jnp.float32)
        expert_hidden = (jax.nn.silu(gate_sum) * up_sum).astype(jnp.bfloat16)
        routed = jnp.dot(expert_hidden, expert_down[0], preferred_element_type=jnp.float32)
    else:
        grid = piece.reshape(ep_count, local_experts, capacity, width)
        gate_sum = jnp.einsum("secd,edf->secf", grid, expert_gate, preferred_element_type=jnp.float32)
        up_sum = jnp.einsum("secd,edf->secf", grid, expert_up, preferred_element_type=jnp.float32)
        expert_hidden = (jax.nn.silu(gate_sum) * up_sum).astype(jnp.bfloat16)
        routed = jnp.einsum(
            "secf,efd->secd", expert_hidden, expert_down, preferred_element_type=jnp.float32
        ).reshape(slots, width)
    summed = scatter_sum(jnp.concatenate([routed, common], axis=0).astype(jnp.bfloat16))
    returned = lax.all_to_all(
        summed[:slots].astype(jnp.bfloat16), "ep", split_axis=0, concat_axis=0, tiled=True
    )
    gates = route_scores / jnp.sum(route_scores, axis=-1, keepdims=True) * ROUTED_SCALE
    mix = summed[slots:]
    for k in range(topk):
        row = jnp.dot(picks[k].astype(jnp.bfloat16), returned, preferred_element_type=jnp.float32)
        mix = mix + row * gates[:, k, None]
    return mix.astype(jnp.bfloat16)


def gather_pieces(piece):
    held = {0: piece}
    for bit in reversed(range(lax.axis_size("tp").bit_length() - 1)):
        for mask, part in list(held.items()):
            held[mask | 1 << bit] = swap(part, "tp", 1 << bit)
    return [held[mask] for mask in range(len(held))]


def near_kernel(kept_ref, got_ref, stay_ref, leave_ref):
    far = lax.axis_index("tp") // 2
    stay_ref[...] = kept_ref[far].astype(jnp.float32) + got_ref[far].astype(jnp.float32)
    away = kept_ref[1 - far].astype(jnp.float32) + got_ref[1 - far].astype(jnp.float32)
    leave_ref[...] = away.astype(leave_ref.dtype)


def far_kernel(stay_ref, got_ref, routed_ref, common_ref):
    slots = routed_ref.shape[0]
    total = stay_ref[...] + got_ref[...].astype(jnp.float32)
    routed_ref[...] = total[:slots].astype(routed_ref.dtype)
    common_ref[...] = total[slots:]


def scatter_rest(kept, sent, slots):
    _, rows, cols = kept.shape
    vmem = pl.BlockSpec(memory_space=pltpu.VMEM)
    cost = pl.CostEstimate(
        flops=4 * rows * cols, bytes_accessed=12 * rows * cols, transcendentals=0
    )
    got = swap(sent, "tp", 1)
    stay, leave = pl.pallas_call(
        near_kernel,
        out_shape=[
            jax.ShapeDtypeStruct((rows, cols), jnp.float32),
            jax.ShapeDtypeStruct((rows, cols), jnp.bfloat16),
        ],
        in_specs=[vmem] * 2,
        out_specs=[vmem] * 2,
        cost_estimate=cost,
        name="near",
    )(kept, got)
    got = swap(leave, "tp", 2)
    return pl.pallas_call(
        far_kernel,
        out_shape=[
            jax.ShapeDtypeStruct((slots, cols), jnp.bfloat16),
            jax.ShapeDtypeStruct((rows - slots, cols), jnp.float32),
        ],
        in_specs=[vmem] * 2,
        out_specs=[vmem] * 2,
        cost_estimate=cost,
        compiler_params=pltpu.CompilerParams(vmem_limit_bytes=8 * MIB),
        name="far",
    )(stay, got)


def route_kernel(capacity, input_ref, gain_ref, ids_ref, out_ref, normed_ref, slots_ref):
    tokens, _ = input_ref.shape
    slots, cols = out_ref.shape
    topk = ids_ref.shape[0]
    inputs = input_ref[...].astype(jnp.float32)
    mean = jnp.mean(inputs * inputs, axis=-1, keepdims=True)
    normed_ref[...] = (inputs * lax.rsqrt(mean + EPS_NORM) * gain_ref[...]).astype(jnp.bfloat16)
    experts_at = -(-(slots // capacity) // 16) * 16
    expert = lax.broadcasted_iota(jnp.int32, (experts_at, tokens), 0)
    named = [ids_ref[k : k + 1] == expert for k in range(topk)]
    count = functools.reduce(jnp.add, [jnp.where(n, 1.0, 0.0) for n in named]).astype(jnp.bfloat16)
    row = lax.broadcasted_iota(jnp.int32, (tokens, tokens), 0)
    column = lax.broadcasted_iota(jnp.int32, (tokens, tokens), 1)
    before = jnp.where(row < column, 1.0, 0.0).astype(jnp.bfloat16)
    earlier = jnp.dot(count, before, preferred_element_type=jnp.float32)
    slot_at = lax.broadcasted_iota(jnp.int32, (slots, tokens), 0)
    taken = None
    for k in range(topk):
        place = jnp.sum(jnp.where(named[k], earlier, 0.0), axis=0, keepdims=True)
        slot = ids_ref[k : k + 1] * capacity + place.astype(jnp.int32)
        slots_ref[k : k + 1] = slot
        taken = slot_at == slot if taken is None else taken | (slot_at == slot)
    own = normed_ref[:, pl.ds(pl.multiple_of(lax.axis_index("tp") * cols, cols), cols)]
    out_ref[...] = jnp.dot(
        jnp.where(taken, 1.0, 0.0).astype(jnp.bfloat16), own, preferred_element_type=jnp.float32
    ).astype(out_ref.dtype)


def route(moe_input, moe_gain, route_ids, capacity, slots, cols):
    tokens, width = moe_input.shape
    vmem = pl.BlockSpec(memory_space=pltpu.VMEM)
    return pl.pallas_call(
        functools.partial(route_kernel, capacity),
        out_shape=[
            jax.ShapeDtypeStruct((slots, cols), jnp.bfloat16),
            jax.ShapeDtypeStruct((tokens, width), jnp.bfloat16),
            jax.ShapeDtypeStruct(route_ids.shape, jnp.int32),
        ],
        in_specs=[vmem] * 3,
        out_specs=[vmem] * 3,
        cost_estimate=pl.CostEstimate(
            flops=2 * slots * tokens * cols, bytes_accessed=6 * moe_input.size, transcendentals=tokens
        ),
        name="route",
    )(moe_input, moe_gain.reshape(1, width), route_ids)


def silu_product(gate_sum, up_sum):
    return (gate_sum / (1.0 + jnp.exp(-gate_sum)) * up_sum).astype(jnp.bfloat16)


def experts_kernel(shared_ref, shared_down_ref, gate_ref, up_ref, down_ref, *refs):
    pieces, (kept_ref, sent_ref) = refs[:-2], refs[-2:]
    tp_index = lax.axis_index("tp")
    core = lax.rem(tp_index, 2)
    slots, cols = pieces[0].shape
    gate_sum = up_sum = None
    for mask, piece in enumerate(pieces):
        at = pl.ds(pl.multiple_of((tp_index ^ mask) * cols, cols), cols)
        gate = jnp.dot(piece[...], gate_ref[0, at], preferred_element_type=jnp.float32)
        up = jnp.dot(piece[...], up_ref[0, at], preferred_element_type=jnp.float32)
        gate_sum = gate if gate_sum is None else gate_sum + gate
        up_sum = up if up_sum is None else up_sum + up
    hidden = silu_product(gate_sum, up_sum)
    for far in range(kept_ref.shape[0]):
        for ref, near in ((kept_ref, core), (sent_ref, 1 - core)):
            at = pl.ds(pl.multiple_of((2 * far + near) * cols, cols), cols)
            ref[far, :slots] = jnp.dot(
                hidden, down_ref[0, :, at], preferred_element_type=jnp.float32
            ).astype(ref.dtype)
            ref[far, slots:] = jnp.dot(
                shared_ref[...], shared_down_ref[:, at], preferred_element_type=jnp.float32
            ).astype(ref.dtype)


def experts(shared_hidden, shared_down, gate, up, down, pieces):
    slots, cols = pieces[0].shape
    rows = slots + shared_hidden.shape[0]
    vmem = pl.BlockSpec(memory_space=pltpu.VMEM)
    shape = jax.ShapeDtypeStruct((len(pieces) // 2, rows, cols), jnp.bfloat16)
    return pl.pallas_call(
        experts_kernel,
        out_shape=[shape, shape],
        in_specs=[vmem] * (5 + len(pieces)),
        out_specs=[vmem, vmem],
        cost_estimate=pl.CostEstimate(
            flops=6 * slots * gate.size + 2 * shared_hidden.size * shared_down.shape[1],
            bytes_accessed=2 * (3 * gate.size + shared_down.size + 2 * rows * cols * len(pieces)),
            transcendentals=slots * gate.shape[2],
        ),
        compiler_params=pltpu.CompilerParams(vmem_limit_bytes=30 * MIB),
        name="experts",
    )(shared_hidden, shared_down, gate, up, down, *pieces)


def combine_kernel(common_ref, returned_ref, slots_ref, scores_ref, out_ref):
    scores = scores_ref[...]
    gates = scores / jnp.sum(scores, axis=0, keepdims=True) * ROUTED_SCALE
    tokens = out_ref.shape[0]
    slot_at = lax.broadcasted_iota(jnp.int32, (returned_ref.shape[0], tokens), 0)
    share = jnp.zeros(slot_at.shape, jnp.float32)
    for k in range(scores.shape[0]):
        share = share + jnp.where(slot_at == slots_ref[k : k + 1], gates[k : k + 1], 0.0)
    high = share.astype(jnp.bfloat16)
    low = (share - high.astype(jnp.float32)).astype(jnp.bfloat16)
    mix = common_ref[...]
    for part in (high, low):
        mix = mix + lax.dot_general(
            part, returned_ref[...], (((0,), (0,)), ((), ())), preferred_element_type=jnp.float32
        )
    out_ref[...] = mix.astype(out_ref.dtype)


def combine(common, returned, slot_ids, route_scores):
    vmem = pl.BlockSpec(memory_space=pltpu.VMEM)
    return pl.pallas_call(
        combine_kernel,
        out_shape=jax.ShapeDtypeStruct(common.shape, jnp.bfloat16),
        in_specs=[vmem] * 4,
        out_specs=vmem,
        cost_estimate=pl.CostEstimate(
            flops=4 * common.size * returned.shape[0],
            bytes_accessed=6 * common.size + 2 * returned.size,
            transcendentals=0,
        ),
        compiler_params=pltpu.CompilerParams(vmem_limit_bytes=8 * MIB),
        name="combine",
    )(common, returned, slot_ids, route_scores)


def expert_layer_near(
    moe_input,
    moe_gain,
    route_ids,
    route_scores,
    shared_gate,
    shared_up,
    shared_down,
    expert_gate,
    expert_up,
    expert_down,
):
    ep_count = lax.axis_size("ep")
    token_count, width = moe_input.shape
    cols = width // lax.axis_size("tp")
    expert_count = expert_gate.shape[0] * ep_count
    capacity = 3 * token_count * route_ids.shape[1] // (2 * expert_count)
    slots = expert_count * capacity
    outgoing, normed, slot_ids = route(
        moe_input, moe_gain, route_ids.T, capacity, slots, cols
    )
    arrived = lax.all_to_all(outgoing, "ep", split_axis=0, concat_axis=0, tiled=True)
    pieces = gather_pieces(arrived)
    shared_hidden = silu_product(
        jnp.dot(normed, shared_gate, preferred_element_type=jnp.float32),
        jnp.dot(normed, shared_up, preferred_element_type=jnp.float32),
    )
    kept, sent = experts(
        shared_hidden, shared_down, expert_gate, expert_up, expert_down, pieces
    )
    routed, common = scatter_rest(kept, sent, slots)
    returned = lax.all_to_all(routed, "ep", split_axis=0, concat_axis=0, tiled=True)
    return combine(common, returned, slot_ids, route_scores.T)


def body(queries, keys, values, key_bias, out_weight, *moe):
    ep_count, tp_count = lax.axis_size("ep"), lax.axis_size("tp")
    span, width = queries.shape
    heads = key_bias.shape[1]
    cols = out_weight.shape[1] // tp_count
    tokens = moe[0].shape[0]
    slots = 3 * tokens * moe[2].shape[1] // 2
    aligned = span % 512 == 0 and width % (128 * heads) == 0 and cols % 256 == 0 and slots % 16 == 0
    near = SEQUENCE_COUNT == 1 and 2 * heads == ep_count and tp_count == 4 and aligned
    if not near or ep_count % 4 or moe[7].shape[0] != 1 or slots % ep_count or tokens % 128:
        return (
            row_attention(queries, keys, values, key_bias, out_weight),
            expert_layer(*moe),
        )
    messages = pack(keys, values, queries, key_bias.T)
    mixed = head_attention(messages, out_weight, heads)
    return (mixed, expert_layer_near(*moe))


def solution(mesh):
    return jax.shard_map(
        body,
        mesh=mesh,
        in_specs=(
            P("ep", "tp"),
            P("ep", "tp"),
            P("ep", "tp"),
            P("ep", "tp"),
            P("tp", None),
            P("ep", None),
            P(),
            P("ep", None),
            P("ep", None),
            P(None, "tp"),
            P(None, "tp"),
            P("tp", None),
            P("ep", None, "tp"),
            P("ep", None, "tp"),
            P("ep", "tp", None),
        ),
        out_specs=(P("ep", "tp"), P("ep", "tp")),
        check_vma=False,
    )
```

```python
import functools

import jax
import jax.numpy as jnp
import numpy as np
from jax import lax
from jax.experimental import pallas as pl
from jax.experimental.pallas import tpu as pltpu
from jax.sharding import PartitionSpec as P


SEQUENCE_COUNT = 1


EPS_NORM = 1e-06
ROUTED_SCALE = 2.5
LOG2E = 1.4426950408889634
NEVER = -1e30
MIB = 1 << 20


def partner_2(array, axis, apart):
    return lax.ppermute(array, axis, [(i, i ^ 1 << apart) for i in range(lax.axis_size(axis))])


def swap(array, axis, mask):
    return lax.ppermute(array, axis, [(i, i ^ mask) for i in range(lax.axis_size(axis))])


def rounds_of(heads):
    return [(k, s) for k in range(heads) for s in range(2)]


def send_round(array, heads, k, s):
    ep_count, tp_count = lax.axis_size("ep"), lax.axis_size("tp")
    pairs = []
    for i in range(ep_count):
        for t in range(tp_count):
            core = t % 2
            to_ep = core * heads + (i + k) % heads
            to_tp = t - core + (i // heads + s) % 2
            pairs.append((i * tp_count + t, to_ep * tp_count + to_tp))
    return lax.ppermute(array, ("ep", "tp"), pairs)


def pack_kernel(heads, k_ref, v_ref, q_ref, bias_ref, *refs):
    out_refs, bias_s = refs[:-1], refs[-1]
    own = lax.axis_index("ep")
    span = k_ref.shape[0]
    half = span // 2
    depth = k_ref.shape[1] // heads
    bias_rows = half // depth
    turned = bias_ref[...].astype(jnp.float32)
    for head in range(heads):
        for r in range(span // depth):
            bias_s[head, r] = turned[head : head + 1, r * depth : (r + 1) * depth]
    for (k, s), out_ref in zip(rounds_of(heads), out_refs):
        head = lax.rem(own + k, heads)
        part = lax.rem(own // heads + s, 2)
        rows = pl.ds(pl.multiple_of(part * half, half), half)
        lanes = pl.ds(pl.multiple_of(head * depth, depth), depth)
        out_ref[:half] = k_ref[rows, lanes]
        out_ref[half : 2 * half] = v_ref[rows, lanes]
        pad = out_ref.shape[0] - 3 * half
        at = lax.broadcasted_iota(jnp.int32, (pad, depth), 0)
        bias = jnp.zeros((pad, depth), jnp.float32)
        for r in range(bias_rows):
            bias = jnp.where(at == r, bias_s[head, part * bias_rows + r], bias)
        out_ref[2 * half : 2 * half + pad] = bias.astype(out_ref.dtype)
        out_ref[2 * half + pad :] = q_ref[rows, lanes]


def pack(keys, values, queries, bias):
    heads, span = bias.shape
    half, depth = span // 2, keys.shape[1] // heads
    pad = -(-(half // depth) // 16) * 16
    vmem = pl.BlockSpec(memory_space=pltpu.VMEM)
    count = len(rounds_of(heads))
    shape = jax.ShapeDtypeStruct((3 * half + pad, depth), keys.dtype)
    return pl.pallas_call(
        functools.partial(pack_kernel, heads),
        out_shape=[shape] * count,
        in_specs=[vmem] * 4,
        out_specs=[vmem] * count,
        scratch_shapes=[pltpu.VMEM((heads, span // depth, 1, depth), jnp.float32)],
        cost_estimate=pl.CostEstimate(
            flops=keys.size * 8, bytes_accessed=12 * keys.size, transcendentals=0
        ),
        name="pack",
    )(keys, values, queries, bias)


def steps_of(blocks):
    steps = [(block, source) for block in range(blocks) for source in reversed(range(block + 1))]
    return steps + [(blocks, 0)] * (2 + len(steps) % 2)


def stick_kernel(scale, heads, turns, spot, table_ref, *refs):
    count = 2 * heads
    messages, out_refs = refs[: 2 * count], refs[2 * count : 2 * count + turns]
    mes_s, q_s, b_s, tri_s, reach_s, soft_s, log_s, prod_s, acc_s, carry_s, sems = refs[
        2 * count + turns :
    ]
    _, blocks, length, width = mes_s.shape
    rows = turns * out_refs[0].shape[1]
    bias_rows = rows // width
    pad = length - 3 * rows
    place, mine = spot()
    for at, which in enumerate((mine, 1 - mine)):
        for (k, s), ref in zip(rounds_of(heads), messages[at * count : (at + 1) * count]):
            block = lax.rem(which + s, 2) * heads + lax.rem(place + heads - k, heads)
            pltpu.make_async_copy(ref, mes_s.at[which, block], sems.at[which, block]).start()
    later = lax.broadcasted_iota(jnp.int32, (2 * rows, rows), 0)
    column = lax.broadcasted_iota(jnp.int32, (2 * rows, rows), 1)
    tri_s[...] = jnp.where(later > column, 1.0, 0.0).astype(jnp.bfloat16)
    row = lax.broadcasted_iota(jnp.int32, (rows, rows), 0)
    reach_s[...] = lax.broadcasted_iota(jnp.int32, (rows, rows), 1) - row - mine * rows
    for block in range(blocks):
        for which in (0, 1):
            pltpu.make_async_copy(messages[0], mes_s.at[which, block], sems.at[which, block]).wait()
            lanes = [
                mes_s[which, block, 2 * rows + r : 2 * rows + r + 1, :].astype(jnp.float32)
                for r in range(bias_rows)
            ]
            b_s[which, block] = jnp.concatenate(lanes, axis=1) * LOG2E
        q_s[block] = mes_s[mine, block, 2 * rows + pad :]
    q_s[blocks] = q_s[0]
    parts = (1, 0)

    def scores(block, source):
        return [
            lax.dot_general(
                q_s[block],
                mes_s[part, source, :rows],
                (((1,), (1,)), ((), ())),
                preferred_element_type=jnp.float32,
            )
            for part in parts
        ]

    def soften(slot, block, source):
        ahead = (block - source) * (2 * rows)
        for part in parts:
            logit = prod_s[part] * scale + b_s[part, source]
            logit = jnp.where(reach_s[...] < ahead - part * rows, logit, NEVER)
            soft = jnp.maximum(logit, jnp.log2(1.0 + jnp.exp2(jnp.minimum(logit, 64.0))))
            soft_s[slot, part] = soft.astype(jnp.bfloat16)
            log_s[slot, part] = logit - soft

    def sums(slot):
        one = jnp.dot(soft_s[slot, 1], tri_s[:rows], preferred_element_type=jnp.float32)
        both = jnp.concatenate([soft_s[slot, 0], soft_s[slot, 1]], axis=1)
        return [one, jnp.dot(both, tri_s[...], preferred_element_type=jnp.float32)]

    def entry(t):
        return table_ref[0, 2 * t], table_ref[0, 2 * t + 1]

    def put(products):
        for part, product in zip(parts, products):
            prod_s[part] = product

    put(scores(*entry(0)))
    soften(0, *entry(0))
    put(scores(*entry(1)))

    def pair(at, _):
        acc = acc_s[...]
        carry = carry_s[...]
        for slot in range(2):
            t = 2 * at + slot
            soften(1 - slot, *entry(t + 1))
            products = scores(*entry(t + 2))
            totals = sums(slot)
            put(products)
            wide = jnp.concatenate([carry] * bias_rows, axis=1)
            block, source = entry(t)
            for part, total in zip(parts, totals):
                weight = jnp.exp2(log_s[slot, part] - (total + wide)).astype(jnp.bfloat16)
                values = mes_s[part, source, rows : 2 * rows]
                acc = acc + jnp.dot(weight, values, preferred_element_type=jnp.float32)
            whole = totals[1][:, :1] + soft_s[slot, 0, :, :width].astype(jnp.float32)[:, :1]
            carry = carry + jnp.broadcast_to(whole, (rows, width))
            for turn, out_ref in enumerate(out_refs):
                piece = out_ref.shape[1]
                out_ref[block] = acc[turn * piece : (turn + 1) * piece].astype(out_ref.dtype)
            more = source > 0
            acc = jnp.where(more, acc, 0.0)
            carry = jnp.where(more, carry, 0.0)
        acc_s[...] = acc
        carry_s[...] = carry
        return 0

    acc_s[...] = jnp.zeros_like(acc_s)
    carry_s[...] = jnp.zeros_like(carry_s)
    pairs = table_ref.shape[1] // 4 - 1
    unroll = max(u for u in range(1, 10) if pairs % u == 0)
    lax.fori_loop(0, pairs, pair, 0, unroll=unroll)


def here():
    return lax.axis_index("ep"), lax.rem(lax.axis_index("tp"), 2)


def stick(own, other, blocks, rows, width, turns, spot=here):
    length = own[0].shape[0]
    table = np.array(steps_of(blocks), np.int32).reshape(1, -1)
    pairs = 2 * rows * rows * (table.shape[1] // 2 - 2)
    shape = jax.ShapeDtypeStruct((blocks, rows // turns, width), jnp.bfloat16)
    return pl.pallas_call(
        functools.partial(stick_kernel, width**-0.5 * LOG2E, len(own) // 2, turns, spot),
        out_shape=[shape] * turns,
        in_specs=[pl.BlockSpec(memory_space=pltpu.SMEM)]
        + [pl.BlockSpec(memory_space=pl.ANY)] * (2 * len(own)),
        out_specs=[pl.BlockSpec(memory_space=pltpu.VMEM)] * turns,
        scratch_shapes=[
            pltpu.VMEM((2, blocks, length, width), jnp.bfloat16),
            pltpu.VMEM((blocks + 1, rows, width), jnp.bfloat16),
            pltpu.VMEM((2, blocks, 1, rows), jnp.float32),
            pltpu.VMEM((2 * rows, rows), jnp.bfloat16),
            pltpu.VMEM((rows, rows), jnp.int32),
            pltpu.VMEM((2, 2, rows, rows), jnp.bfloat16),
            pltpu.VMEM((2, 2, rows, rows), jnp.float32),
            pltpu.VMEM((2, rows, rows), jnp.float32),
            pltpu.VMEM((rows, width), jnp.float32),
            pltpu.VMEM((rows, width), jnp.float32),
            pltpu.SemaphoreType.DMA((2, blocks)),
        ],
        cost_estimate=pl.CostEstimate(
            flops=2 * pairs * (rows + 3 * width),
            bytes_accessed=10 * blocks * rows * width,
            transcendentals=3 * pairs,
        ),
        name="stick",
    )(jnp.asarray(table), *own, *other)


def project_kernel(masks, own_ref, other_ref, *refs):
    count = len(masks)
    back_refs, out_refs = refs[: -count - 3], refs[-count - 3 : -3]
    rows_s, weight_s, sems = refs[-3:]
    ep_index, tp_index = lax.axis_index("ep"), lax.axis_index("tp")
    core = lax.rem(tp_index, 2)
    width = own_ref.shape[0]
    cols = out_refs[0].shape[1]
    copies = []
    for at, mask in enumerate(masks):
        columns = pl.ds(pl.multiple_of((tp_index ^ mask) * cols, cols), cols)
        for which, ref in enumerate((own_ref, other_ref)):
            copy = pltpu.make_async_copy(
                ref.at[:, columns], weight_s.at[at, which], sems.at[at, which]
            )
            copy.start()
            copies.append(copy)
    depth = back_refs[0].shape[-1]
    heads = rows_s.shape[1] // depth
    for head in range(heads):
        if len(back_refs) == 1:
            rows_s[:, head * depth : (head + 1) * depth] = back_refs[0][head]
        else:
            at = pl.ds(pl.multiple_of((ep_index ^ head) * depth, depth), depth)
            ref = back_refs[head]
            rows_s[:, at] = ref[...] if head else ref[ep_index]
    own_rows = rows_s[:, pl.ds(pl.multiple_of(core * width, width), width)]
    other_rows = rows_s[:, pl.ds(pl.multiple_of((1 - core) * width, width), width)]
    for at, out_ref in enumerate(out_refs):
        copies[2 * at].wait()
        part = jnp.dot(own_rows, weight_s[at, 0], preferred_element_type=jnp.float32)
        copies[2 * at + 1].wait()
        part += jnp.dot(other_rows, weight_s[at, 1], preferred_element_type=jnp.float32)
        out_ref[...] = part.astype(out_ref.dtype)


def project(back, own_weight, other_weight, tp_count, masks):
    rows = back[0].shape[1]
    cols = own_weight.shape[1] // tp_count
    vmem = pl.BlockSpec(memory_space=pltpu.VMEM)
    shape = jax.ShapeDtypeStruct((rows, cols), jnp.bfloat16)
    return pl.pallas_call(
        functools.partial(project_kernel, masks),
        out_shape=[shape] * len(masks),
        in_specs=[pl.BlockSpec(memory_space=pl.ANY)] * 2 + [vmem] * len(back),
        out_specs=[vmem] * len(masks),
        scratch_shapes=[
            pltpu.VMEM((rows, 2 * own_weight.shape[0]), jnp.bfloat16),
            pltpu.VMEM((len(masks), 2, own_weight.shape[0], cols), jnp.bfloat16),
            pltpu.SemaphoreType.DMA((len(masks), 2)),
        ],
        cost_estimate=pl.CostEstimate(
            flops=4 * rows * own_weight.size * len(masks) // tp_count,
            bytes_accessed=4 * own_weight.size + 4 * rows * own_weight.shape[1],
            transcendentals=0,
        ),
        compiler_params=pltpu.CompilerParams(vmem_limit_bytes=16 * MIB),
        name="project",
    )(own_weight, other_weight, *back)


def finish_kernel(turns, *refs):
    out_ref = refs[-1]
    core = lax.rem(lax.axis_index("tp"), 2)
    piece = refs[0].shape[0]
    count = (len(refs) - 1) // turns
    for turn in range(turns):
        for bit in range(2):
            mine = [ref[...].astype(jnp.float32) for ref in refs[turn * count + bit : (turn + 1) * count : 2]]
            total = functools.reduce(jnp.add, mine)
            part = core if bit == 0 else 1 - core
            at = pl.multiple_of((part * turns + turn) * piece, piece)
            out_ref[pl.ds(at, piece)] = total.astype(out_ref.dtype)


def finish(pieces):
    turns = len(pieces)
    flat = sum(pieces, [])
    rows, cols = flat[0].shape
    vmem = pl.BlockSpec(memory_space=pltpu.VMEM)
    return pl.pallas_call(
        functools.partial(finish_kernel, turns),
        out_shape=jax.ShapeDtypeStruct((2 * turns * rows, cols), jnp.bfloat16),
        in_specs=[vmem] * len(flat),
        out_specs=vmem,
        cost_estimate=pl.CostEstimate(
            flops=8 * rows * turns * cols, bytes_accessed=12 * rows * turns * cols, transcendentals=0
        ),
        compiler_params=pltpu.CompilerParams(vmem_limit_bytes=8 * MIB),
        name="finish",
    )(*flat)


TURNS = 1


def head_attention(messages, out_weight, heads):
    ep_count = lax.axis_size("ep")
    tp_count = lax.axis_size("tp")
    own, other = [], []
    for (k, s), message in zip(rounds_of(heads), messages):
        own.append(send_round(message, heads, k, s))
        other.append(swap(own[-1], "tp", 1))
    depth = out_weight.shape[0] // heads
    half = messages[0].shape[0] // 3 // 16 * 16
    other_weight = swap(out_weight, "tp", 1)
    outs = stick(own, other, ep_count, half, depth, TURNS)
    backs = []
    backs.append([lax.all_to_all(outs[0], "ep", split_axis=0, concat_axis=0, tiled=True)])
    ep_index = lax.axis_index("ep")
    for turn in range(1, TURNS):
        back = [outs[turn]]
        for mask in range(1, ep_count):
            row = lax.dynamic_index_in_dim(outs[turn], ep_index ^ mask, 0, False)
            back.append(swap(row, "ep", mask))
        backs.append(back)
    pieces = []
    for back in backs:
        parts = {}
        for masks in (range(tp_count - 1, 1, -1), (1, 0)):
            made = project(back, out_weight, other_weight, tp_count, tuple(masks))
            for mask, part in zip(masks, made):
                parts[mask] = swap(part, "tp", mask) if mask else part
        pieces.append([parts[mask] for mask in range(tp_count)])
    return finish(pieces)


def absorb(state, query_heads, piece, visible):
    total, carried = state
    key_piece, value_piece, bias_piece = piece
    span = key_piece.shape[0]
    heads = query_heads.shape[1]
    key_heads = key_piece.reshape(span, heads, -1)
    value_heads = value_piece.reshape(span, heads, -1)
    scale = query_heads.shape[2] ** (-0.5)
    logit = (
        jnp.einsum("qhd,khd->hqk", query_heads, key_heads, preferred_element_type=jnp.float32)
        * scale
    )
    logit = logit + bias_piece.astype(jnp.float32).T[:, None, :]
    keep = jnp.where(visible[None], jax.nn.log_sigmoid(-logit), 0.0)
    stay = lax.cumsum(keep, axis=2, reverse=True) - keep + carried[:, :, None]
    weight = jnp.where(visible[None], jnp.exp(jax.nn.log_sigmoid(logit) + stay), 0.0).astype(
        jnp.bfloat16
    )
    total = total + jnp.einsum(
        "hqk,khd->qhd", weight, value_heads, preferred_element_type=jnp.float32
    )
    return (total, carried + jnp.sum(keep, axis=2))


def fresh_state(query_heads):
    return (
        jnp.zeros(query_heads.shape, jnp.float32),
        jnp.zeros((query_heads.shape[1], query_heads.shape[0]), jnp.float32),
    )


def diagonal(query_heads, piece, offset):
    count = query_heads.shape[0]
    span = piece[0].shape[0]
    key_pos = jnp.arange(span, dtype=jnp.int32)
    query_pos = offset + jnp.arange(count, dtype=jnp.int32)
    visible = key_pos[None, :] < query_pos[:, None]
    return absorb(fresh_state(query_heads), query_heads, piece, visible)


def row_attention(queries, keys, values, key_bias, out_weight):
    span = queries.shape[0]
    heads = key_bias.shape[1]
    query_heads = queries.reshape(span, heads, -1)
    ep_count = lax.axis_size("ep")
    seq_devices = ep_count // SEQUENCE_COUNT
    own_index = lax.axis_index("ep")
    place = own_index % seq_devices
    own_piece = (keys, values, key_bias)
    half = span // 2
    group_bits = seq_devices.bit_length() - 1

    def mirror(rows):
        for bit in range(group_bits):
            rows = partner_2(rows, "ep", bit)
        return rows

    whole = (
        lax.all_gather(own_piece[0], "ep", axis=0, tiled=True),
        lax.all_gather(own_piece[1], "ep", axis=0, tiled=True),
        lax.all_gather(own_piece[2], "ep", axis=0, tiled=True),
    )
    mirror_place = seq_devices - 1 - place
    mirror_index = own_index - place + mirror_place
    early_rows = query_heads[:half]
    late_rows = mirror(queries[half:]).reshape(half, heads, -1)
    partner = tuple(
        (lax.dynamic_slice_in_dim(member, mirror_index * span, span, 0) for member in whole)
    )
    half_visible = jnp.ones((half, span), jnp.bool_)

    def unchanged(inner):
        return inner

    def visit_both(turn, carry):
        early, late = carry
        early_source = jnp.maximum(own_index - turn, 0)
        late_source = jnp.maximum(mirror_index - turn, 0)
        early_piece = tuple(
            (lax.dynamic_slice_in_dim(member, early_source * span, span, 0) for member in whole)
        )
        late_piece = tuple(
            (lax.dynamic_slice_in_dim(member, late_source * span, span, 0) for member in whole)
        )

        def early_taken(inner):
            return absorb(inner, early_rows, early_piece, half_visible)

        def late_taken(inner):
            return absorb(inner, late_rows, late_piece, half_visible)

        early = lax.cond(place >= turn, early_taken, unchanged, early)
        late = lax.cond(mirror_place >= turn, late_taken, unchanged, late)
        return (early, late)

    early_state, late_state = lax.fori_loop(
        1,
        seq_devices,
        visit_both,
        (diagonal(early_rows, own_piece, 0), diagonal(late_rows, partner, half)),
    )
    early_out = early_state[0].astype(jnp.bfloat16).reshape(half, -1)
    late_out = mirror(late_state[0].astype(jnp.bfloat16).reshape(half, -1))
    heads_out = jnp.concatenate([early_out, late_out], axis=0)
    summed = lax.psum_scatter(
        jnp.dot(heads_out, out_weight, preferred_element_type=jnp.float32).astype(jnp.bfloat16),
        "tp",
        scatter_dimension=1,
        tiled=True,
    )
    return summed


def gather_columns(piece):
    count = lax.axis_size("tp")
    index = lax.axis_index("tp")
    cols = piece.shape[1]
    whole = jnp.zeros((piece.shape[0], count * cols), piece.dtype)
    held = [(0, piece)]
    for bit in reversed(range(count.bit_length() - 1)):
        held = held + [(mask | 1 << bit, swap(part, "tp", 1 << bit)) for mask, part in held]
    for mask, part in held:
        whole = lax.dynamic_update_slice(whole, part, (0, (index ^ mask) * cols))
    return whole


def scatter_sum(partial):
    count = lax.axis_size("tp")
    index = lax.axis_index("tp")
    rows = partial.shape[0]
    parts = partial.reshape(rows, count, -1)
    for bit in range(count.bit_length() - 1):
        mine = index >> bit & 1
        parts = parts.reshape(rows, parts.shape[1] // 2, 2, parts.shape[2])
        kept = lax.dynamic_index_in_dim(parts, mine, 2, False)
        sent = lax.dynamic_index_in_dim(parts, 1 - mine, 2, False)
        parts = kept.astype(jnp.float32) + swap(sent.astype(jnp.bfloat16), "tp", 1 << bit)
    return parts.reshape(rows, -1)


def expert_layer(
    moe_input,
    moe_gain,
    route_ids,
    route_scores,
    shared_gate,
    shared_up,
    shared_down,
    expert_gate,
    expert_up,
    expert_down,
):
    ep_count = lax.axis_size("ep")
    token_count, width = moe_input.shape
    cols = width // lax.axis_size("tp")
    inputs = moe_input.astype(jnp.float32)
    normed = (
        inputs * lax.rsqrt(jnp.mean(inputs * inputs, axis=-1, keepdims=True) + EPS_NORM) * moe_gain
    ).astype(jnp.bfloat16)
    own_cols = lax.dynamic_slice_in_dim(normed, lax.axis_index("tp") * cols, cols, 1)
    local_experts = expert_gate.shape[0]
    expert_count = local_experts * ep_count
    topk = route_ids.shape[1]
    capacity = 3 * token_count * topk // (2 * expert_count)
    slots = expert_count * capacity
    pairs = token_count * topk
    chosen = route_ids.reshape(-1)
    pair_at = jnp.arange(pairs, dtype=jnp.int32)
    earlier = (chosen[:, None] == chosen[None, :]) & (pair_at[None, :] < pair_at[:, None])
    place_in = jnp.sum(earlier.astype(jnp.int32), axis=1)
    slot_ids = (chosen * capacity + place_in).reshape(token_count, topk)
    slot_at = jnp.arange(slots, dtype=jnp.int32)
    picks = [(slot_ids[:, k, None] == slot_at[None, :]) for k in range(topk)]
    dispatch = functools.reduce(jnp.logical_or, picks).astype(jnp.bfloat16)
    outgoing = lax.dot_general(
        dispatch, own_cols, (((0,), (0,)), ((), ())), preferred_element_type=jnp.float32
    ).astype(jnp.bfloat16)
    arrived = lax.all_to_all(outgoing, "ep", split_axis=0, concat_axis=0, tiled=True)
    piece = gather_columns(arrived)
    shared_hidden = (
        jax.nn.silu(jnp.dot(normed, shared_gate, preferred_element_type=jnp.float32))
        * jnp.dot(normed, shared_up, preferred_element_type=jnp.float32)
    ).astype(jnp.bfloat16)
    common = jnp.dot(shared_hidden, shared_down, preferred_element_type=jnp.float32)
    if local_experts == 1:
        grid = piece
        gate_sum = jnp.dot(grid, expert_gate[0], preferred_element_type=jnp.float32)
        up_sum = jnp.dot(grid, expert_up[0], preferred_element_type=jnp.float32)
        expert_hidden = (jax.nn.silu(gate_sum) * up_sum).astype(jnp.bfloat16)
        routed = jnp.dot(expert_hidden, expert_down[0], preferred_element_type=jnp.float32)
    else:
        grid = piece.reshape(ep_count, local_experts, capacity, width)
        gate_sum = jnp.einsum("secd,edf->secf", grid, expert_gate, preferred_element_type=jnp.float32)
        up_sum = jnp.einsum("secd,edf->secf", grid, expert_up, preferred_element_type=jnp.float32)
        expert_hidden = (jax.nn.silu(gate_sum) * up_sum).astype(jnp.bfloat16)
        routed = jnp.einsum(
            "secf,efd->secd", expert_hidden, expert_down, preferred_element_type=jnp.float32
        ).reshape(slots, width)
    summed = scatter_sum(jnp.concatenate([routed, common], axis=0).astype(jnp.bfloat16))
    returned = lax.all_to_all(
        summed[:slots].astype(jnp.bfloat16), "ep", split_axis=0, concat_axis=0, tiled=True
    )
    gates = route_scores / jnp.sum(route_scores, axis=-1, keepdims=True) * ROUTED_SCALE
    mix = summed[slots:]
    for k in range(topk):
        row = jnp.dot(picks[k].astype(jnp.bfloat16), returned, preferred_element_type=jnp.float32)
        mix = mix + row * gates[:, k, None]
    return mix.astype(jnp.bfloat16)


def gather_pieces(piece):
    held = {0: piece}
    for bit in reversed(range(lax.axis_size("tp").bit_length() - 1)):
        for mask, part in list(held.items()):
            held[mask | 1 << bit] = swap(part, "tp", 1 << bit)
    return [held[mask] for mask in range(len(held))]


def near_kernel(kept_ref, got_ref, stay_ref, leave_ref):
    far = lax.axis_index("tp") // 2
    stay_ref[...] = kept_ref[far].astype(jnp.float32) + got_ref[far].astype(jnp.float32)
    away = kept_ref[1 - far].astype(jnp.float32) + got_ref[1 - far].astype(jnp.float32)
    leave_ref[...] = away.astype(leave_ref.dtype)


def far_kernel(stay_ref, got_ref, routed_ref, common_ref):
    slots = routed_ref.shape[0]
    total = stay_ref[...] + got_ref[...].astype(jnp.float32)
    routed_ref[...] = total[:slots].astype(routed_ref.dtype)
    common_ref[...] = total[slots:]


def scatter_rest(kept, sent, slots):
    _, rows, cols = kept.shape
    vmem = pl.BlockSpec(memory_space=pltpu.VMEM)
    cost = pl.CostEstimate(
        flops=4 * rows * cols, bytes_accessed=12 * rows * cols, transcendentals=0
    )
    got = swap(sent, "tp", 1)
    stay, leave = pl.pallas_call(
        near_kernel,
        out_shape=[
            jax.ShapeDtypeStruct((rows, cols), jnp.float32),
            jax.ShapeDtypeStruct((rows, cols), jnp.bfloat16),
        ],
        in_specs=[vmem] * 2,
        out_specs=[vmem] * 2,
        cost_estimate=cost,
        name="near",
    )(kept, got)
    got = swap(leave, "tp", 2)
    return pl.pallas_call(
        far_kernel,
        out_shape=[
            jax.ShapeDtypeStruct((slots, cols), jnp.bfloat16),
            jax.ShapeDtypeStruct((rows - slots, cols), jnp.float32),
        ],
        in_specs=[vmem] * 2,
        out_specs=[vmem] * 2,
        cost_estimate=cost,
        compiler_params=pltpu.CompilerParams(vmem_limit_bytes=8 * MIB),
        name="far",
    )(stay, got)


def route_kernel(capacity, input_ref, gain_ref, ids_ref, out_ref, normed_ref, slots_ref):
    tokens, _ = input_ref.shape
    slots, cols = out_ref.shape
    topk = ids_ref.shape[0]
    inputs = input_ref[...].astype(jnp.float32)
    mean = jnp.mean(inputs * inputs, axis=-1, keepdims=True)
    normed_ref[...] = (inputs * lax.rsqrt(mean + EPS_NORM) * gain_ref[...]).astype(jnp.bfloat16)
    experts_at = -(-(slots // capacity) // 16) * 16
    expert = lax.broadcasted_iota(jnp.int32, (experts_at, tokens), 0)
    named = [ids_ref[k : k + 1] == expert for k in range(topk)]
    count = functools.reduce(jnp.add, [jnp.where(n, 1.0, 0.0) for n in named]).astype(jnp.bfloat16)
    row = lax.broadcasted_iota(jnp.int32, (tokens, tokens), 0)
    column = lax.broadcasted_iota(jnp.int32, (tokens, tokens), 1)
    before = jnp.where(row < column, 1.0, 0.0).astype(jnp.bfloat16)
    earlier = jnp.dot(count, before, preferred_element_type=jnp.float32)
    slot_at = lax.broadcasted_iota(jnp.int32, (slots, tokens), 0)
    taken = None
    for k in range(topk):
        place = jnp.sum(jnp.where(named[k], earlier, 0.0), axis=0, keepdims=True)
        slot = ids_ref[k : k + 1] * capacity + place.astype(jnp.int32)
        slots_ref[k : k + 1] = slot
        taken = slot_at == slot if taken is None else taken | (slot_at == slot)
    own = normed_ref[:, pl.ds(pl.multiple_of(lax.axis_index("tp") * cols, cols), cols)]
    out_ref[...] = jnp.dot(
        jnp.where(taken, 1.0, 0.0).astype(jnp.bfloat16), own, preferred_element_type=jnp.float32
    ).astype(out_ref.dtype)


def route(moe_input, moe_gain, route_ids, capacity, slots, cols):
    tokens, width = moe_input.shape
    vmem = pl.BlockSpec(memory_space=pltpu.VMEM)
    return pl.pallas_call(
        functools.partial(route_kernel, capacity),
        out_shape=[
            jax.ShapeDtypeStruct((slots, cols), jnp.bfloat16),
            jax.ShapeDtypeStruct((tokens, width), jnp.bfloat16),
            jax.ShapeDtypeStruct(route_ids.shape, jnp.int32),
        ],
        in_specs=[vmem] * 3,
        out_specs=[vmem] * 3,
        cost_estimate=pl.CostEstimate(
            flops=2 * slots * tokens * cols, bytes_accessed=6 * moe_input.size, transcendentals=tokens
        ),
        name="route",
    )(moe_input, moe_gain.reshape(1, width), route_ids)


def silu_product(gate_sum, up_sum):
    return (gate_sum / (1.0 + jnp.exp(-gate_sum)) * up_sum).astype(jnp.bfloat16)


def experts_kernel(shared_ref, shared_down_ref, gate_ref, up_ref, down_ref, *refs):
    pieces, (kept_ref, sent_ref) = refs[:-2], refs[-2:]
    tp_index = lax.axis_index("tp")
    core = lax.rem(tp_index, 2)
    slots, cols = pieces[0].shape
    gate_sum = up_sum = None
    for mask, piece in enumerate(pieces):
        at = pl.ds(pl.multiple_of((tp_index ^ mask) * cols, cols), cols)
        gate = jnp.dot(piece[...], gate_ref[0, at], preferred_element_type=jnp.float32)
        up = jnp.dot(piece[...], up_ref[0, at], preferred_element_type=jnp.float32)
        gate_sum = gate if gate_sum is None else gate_sum + gate
        up_sum = up if up_sum is None else up_sum + up
    hidden = silu_product(gate_sum, up_sum)
    for far in range(kept_ref.shape[0]):
        for ref, near in ((kept_ref, core), (sent_ref, 1 - core)):
            at = pl.ds(pl.multiple_of((2 * far + near) * cols, cols), cols)
            ref[far, :slots] = jnp.dot(
                hidden, down_ref[0, :, at], preferred_element_type=jnp.float32
            ).astype(ref.dtype)
            ref[far, slots:] = jnp.dot(
                shared_ref[...], shared_down_ref[:, at], preferred_element_type=jnp.float32
            ).astype(ref.dtype)


def experts(shared_hidden, shared_down, gate, up, down, pieces):
    slots, cols = pieces[0].shape
    rows = slots + shared_hidden.shape[0]
    vmem = pl.BlockSpec(memory_space=pltpu.VMEM)
    shape = jax.ShapeDtypeStruct((len(pieces) // 2, rows, cols), jnp.bfloat16)
    return pl.pallas_call(
        experts_kernel,
        out_shape=[shape, shape],
        in_specs=[vmem] * (5 + len(pieces)),
        out_specs=[vmem, vmem],
        cost_estimate=pl.CostEstimate(
            flops=6 * slots * gate.size + 2 * shared_hidden.size * shared_down.shape[1],
            bytes_accessed=2 * (3 * gate.size + shared_down.size + 2 * rows * cols * len(pieces)),
            transcendentals=slots * gate.shape[2],
        ),
        compiler_params=pltpu.CompilerParams(vmem_limit_bytes=30 * MIB),
        name="experts",
    )(shared_hidden, shared_down, gate, up, down, *pieces)


def combine_kernel(common_ref, returned_ref, slots_ref, scores_ref, out_ref):
    scores = scores_ref[...]
    gates = scores / jnp.sum(scores, axis=0, keepdims=True) * ROUTED_SCALE
    tokens = out_ref.shape[0]
    slot_at = lax.broadcasted_iota(jnp.int32, (returned_ref.shape[0], tokens), 0)
    share = jnp.zeros(slot_at.shape, jnp.float32)
    for k in range(scores.shape[0]):
        share = share + jnp.where(slot_at == slots_ref[k : k + 1], gates[k : k + 1], 0.0)
    high = share.astype(jnp.bfloat16)
    low = (share - high.astype(jnp.float32)).astype(jnp.bfloat16)
    mix = common_ref[...]
    for part in (high, low):
        mix = mix + lax.dot_general(
            part, returned_ref[...], (((0,), (0,)), ((), ())), preferred_element_type=jnp.float32
        )
    out_ref[...] = mix.astype(out_ref.dtype)


def combine(common, returned, slot_ids, route_scores):
    vmem = pl.BlockSpec(memory_space=pltpu.VMEM)
    return pl.pallas_call(
        combine_kernel,
        out_shape=jax.ShapeDtypeStruct(common.shape, jnp.bfloat16),
        in_specs=[vmem] * 4,
        out_specs=vmem,
        cost_estimate=pl.CostEstimate(
            flops=4 * common.size * returned.shape[0],
            bytes_accessed=6 * common.size + 2 * returned.size,
            transcendentals=0,
        ),
        compiler_params=pltpu.CompilerParams(vmem_limit_bytes=8 * MIB),
        name="combine",
    )(common, returned, slot_ids, route_scores)


def expert_layer_near(
    moe_input,
    moe_gain,
    route_ids,
    route_scores,
    shared_gate,
    shared_up,
    shared_down,
    expert_gate,
    expert_up,
    expert_down,
):
    ep_count = lax.axis_size("ep")
    token_count, width = moe_input.shape
    cols = width // lax.axis_size("tp")
    expert_count = expert_gate.shape[0] * ep_count
    capacity = 3 * token_count * route_ids.shape[1] // (2 * expert_count)
    slots = expert_count * capacity
    outgoing, normed, slot_ids = route(
        moe_input, moe_gain, route_ids.T, capacity, slots, cols
    )
    arrived = lax.all_to_all(outgoing, "ep", split_axis=0, concat_axis=0, tiled=True)
    pieces = gather_pieces(arrived)
    shared_hidden = silu_product(
        jnp.dot(normed, shared_gate, preferred_element_type=jnp.float32),
        jnp.dot(normed, shared_up, preferred_element_type=jnp.float32),
    )
    kept, sent = experts(
        shared_hidden, shared_down, expert_gate, expert_up, expert_down, pieces
    )
    routed, common = scatter_rest(kept, sent, slots)
    returned = lax.all_to_all(routed, "ep", split_axis=0, concat_axis=0, tiled=True)
    return combine(common, returned, slot_ids, route_scores.T)


def body(queries, keys, values, key_bias, out_weight, *moe):
    ep_count, tp_count = lax.axis_size("ep"), lax.axis_size("tp")
    span, width = queries.shape
    heads = key_bias.shape[1]
    cols = out_weight.shape[1] // tp_count
    tokens = moe[0].shape[0]
    slots = 3 * tokens * moe[2].shape[1] // 2
    aligned = span % 512 == 0 and width % (128 * heads) == 0 and cols % 256 == 0 and slots % 16 == 0
    near = SEQUENCE_COUNT == 1 and 2 * heads == ep_count and tp_count == 4 and aligned
    if not near or ep_count % 4 or moe[7].shape[0] != 1 or slots % ep_count or tokens % 128:
        return (
            row_attention(queries, keys, values, key_bias, out_weight),
            expert_layer(*moe),
        )
    messages = pack(keys, values, queries, key_bias.T)
    mixed = head_attention(messages, out_weight, heads)
    return (mixed, expert_layer_near(*moe))


def solution(mesh):
    return jax.shard_map(
        body,
        mesh=mesh,
        in_specs=(
            P("ep", "tp"),
            P("ep", "tp"),
            P("ep", "tp"),
            P("ep", "tp"),
            P("tp", None),
            P("ep", None),
            P(),
            P("ep", None),
            P("ep", None),
            P(None, "tp"),
            P(None, "tp"),
            P("tp", None),
            P("ep", None, "tp"),
            P("ep", None, "tp"),
            P("ep", "tp", None),
        ),
        out_specs=(P("ep", "tp"), P("ep", "tp")),
        check_vma=False,
    )
```
